128 devices in a mesh: sp: 64 (over z, y, x), tp: 2 (over core).
Axes of the slice: x: 4, y: 4, z: 4, core: 2. Of those that a mesh axis runs over, the one named last changes fastest.
Arguments:
- stream_in: bfloat16 [8192, 2048], P(('sp', 'tp')), may hold values from -6 to 6
- query_rows: bfloat16 [8192, 2048], P('sp', 'tp'), may hold values from -6 to 6
- key_rows: bfloat16 [8192, 2048], P('sp', 'tp'), may hold values from -6 to 6
- value_rows: bfloat16 [8192, 2048], P('sp', 'tp'), may hold values from -6 to 6
- removal_key: bfloat16 [8192, 2048], P('sp', 'tp'), may hold values from -6 to 6
- learn_pre: bfloat16 [8192, 2048], P('sp', 'tp'), may hold values from -12 to 4
- log_rate: float32 [8192, 2048], P('sp', 'tp'), may hold values from -14 to 0
- norm_gain: bfloat16 [2048], P('tp'), may hold values from 0.099609375 to 1.8984375
- out_weight: bfloat16 [2048, 2048], replicated, may hold values from -0.125 to 0.125
- ffn_gain: bfloat16 [2048], replicated, may hold values from 0.099609375 to 1.8984375
- routes: int32 [8192, 2], P(('sp', 'tp')), may hold values from 0 to 31, all different within a row; in each aligned block of 64 rows (0 to 63, 64 to 127, ...) at most 8 rows name the same one
- route_weight: float32 [8192, 2], P(('sp', 'tp')), may hold values from 0.1 to 1
- expert_gate: bfloat16 [64, 2048, 1792], P('sp', None, 'tp'), may hold values from -0.125 to 0.125
- expert_up: bfloat16 [64, 2048, 1792], P('sp', None, 'tp'), may hold values from -0.125 to 0.125
- expert_down: bfloat16 [64, 1792, 2048], P('sp', 'tp'), may hold values from -0.09375 to 0.09375
Outputs:
- layer_out: bfloat16 [8192, 2048], P(('sp', 'tp'))
The draws below stay inside these ranges and needn't reach their ends.
Inputs may be any that keep to these rules, and one draw needn't show every extreme that they name: `routes`: in each aligned block of 64 rows (the rows of one device after the mixer) no expert is named by more than 8 rows, a bound that some expert reaches in some or all blocks; the experts of one row differ.
All inputs are finite; a program needn't handle non-finite values.
Results may differ from the reference program's by a relative error of at most 0.0065.
Values may be sent and summed in bfloat16 or wider, within the bound.
A program may use at most 192 MiB of HBM per device.

```python
import math
import jax
import jax.numpy as jnp
import numpy as np
from jax import lax

MODEL_WIDTH = 2048
HEADS = 32
HEAD = 64
FFE = 3584
TOPK = 2
TOK_DEV = 128
SEQUENCE_TOKENS = 8192
HALF = 64
EXPERTS = 32
CAP = 8


def head_kinds(key):
    order = jax.random.permutation(jax.random.fold_in(key, 101), HEADS)
    slow_count = HEADS // 2
    return jnp.repeat((order < slow_count).astype(jnp.float32), HEAD)


def draw_log_rate(key, part):
    lagging_columns = head_kinds(key)
    sequence_lanes = jax.random.split(jax.random.fold_in(key, 202), 6)
    slow_rate = jnp.exp(jax.random.uniform(sequence_lanes[0], (MODEL_WIDTH,), jnp.float32, math.log(0.2), math.log(0.6))) / SEQUENCE_TOKENS
    fast_rate = jnp.exp(-jax.random.uniform(sequence_lanes[1], (MODEL_WIDTH,), jnp.float32, math.log(30.0), math.log(100.0)))
    base_rate = jnp.where(lagging_columns > 0.5, slow_rate, fast_rate)
    block_factor = jnp.exp(jax.random.uniform(sequence_lanes[2], (SEQUENCE_TOKENS // TOK_DEV, 1), jnp.float32, math.log(0.5), math.log(2.0)))
    block_factor = jnp.repeat(block_factor, TOK_DEV, axis=0)
    jitter = jnp.clip(0.4 * jax.random.normal(sequence_lanes[3], (SEQUENCE_TOKENS, MODEL_WIDTH), jnp.float32), -1.2, 1.2)
    decay_rate_table = base_rate[None, :] * block_factor * jnp.exp(jitter)
    surge_positions = jax.random.randint(sequence_lanes[4], (2,), 0, SEQUENCE_TOKENS)
    surge_decay_loss = -jnp.log(jax.random.uniform(sequence_lanes[5], (2, MODEL_WIDTH), jnp.float32, 0.55, 0.8))
    surge_token_hits = (jnp.arange(SEQUENCE_TOKENS)[:, None] == surge_positions[None, :]).astype(jnp.float32)
    decay_rate_table = decay_rate_table + jnp.dot(surge_token_hits, surge_decay_loss) * lagging_columns[None, :]
    return jnp.clip(jnp.log(decay_rate_table), -14.0, 0.0)


def draw_learn_pre(key, part):
    lagging_columns = head_kinds(key)
    sequence_lanes = jax.random.split(jax.random.fold_in(key, 404), 1)
    jitter = jnp.clip(jax.random.normal(sequence_lanes[0], (SEQUENCE_TOKENS, MODEL_WIDTH), jnp.float32), -4.0, 4.0)
    slow_pre = math.log(0.5 * HEAD / SEQUENCE_TOKENS) + 0.5 * jitter
    return jnp.clip(jnp.where(lagging_columns[None, :] > 0.5, slow_pre, jitter), -12.0, 4.0).astype(jnp.bfloat16)


def level_of(own_key, shape, shards, least, top_value):
    gain = 1.0
    for axis_at, parts in shards:
        steps = jax.random.uniform(jax.random.fold_in(jax.random.fold_in(own_key, 6), axis_at), (parts,), jnp.float32, least / len(shards), top_value / len(shards))
        gain = gain * jnp.repeat(jnp.exp(steps), shape[axis_at] // parts).reshape((-1,) + (1,) * (len(shape) - 1 - axis_at))
    return gain


def deal_out(own_key, own, number, rows, number_of, top, most, slope):
    sequence = jax.random.permutation(own_key, number_of)
    crowded, usual = load_shares(number_of, rows * top, most, slope, True), load_shares(number_of, rows * top, most, slope, False)
    places = jnp.arange(number_of)

    def named(lengths, turn):
        used = int((lengths > 0).sum())
        fixed = max(1, used // 4)
        shifted = fixed + (places - fixed + turn * (used - fixed)) % max(1, number_of - fixed)
        return jnp.zeros((number_of,), jnp.int32).at[sequence[jnp.where(places < fixed, places, shifted)]].set(jnp.asarray(lengths, jnp.int32))

    lengths = jnp.where(number % 4 == 0, named(crowded, number // 4), named(usual, number - number // 4 - 1))
    mixed = jax.random.permutation(jax.random.fold_in(own, 3), number_of)
    source_of, sink = mixed[0:number_of // 2 * 2:2], mixed[1:number_of // 2 * 2:2]
    margin = jnp.minimum(lengths[source_of] - 1, most - lengths[sink]) // 2
    margin = jnp.where((source_of == sequence[0]) | (sink == sequence[0]) | (lengths[sink] == 0), 0, jnp.maximum(margin, 0))
    shifted = jax.random.randint(jax.random.fold_in(own, 4), (number_of // 2,), 0, 1 << 20) % (margin + 1)
    lengths = lengths.at[source_of].add(-shifted).at[sink].add(shifted)
    items = jnp.searchsorted(jnp.cumsum(lengths), jnp.arange(rows * top), side="right").astype(jnp.int32)
    table = items.reshape(top, rows).T
    table = table[jax.random.permutation(jax.random.fold_in(own, 1), rows)]
    turn = jax.random.randint(jax.random.fold_in(own, 2), (rows, 1), 0, top)
    return jnp.take_along_axis(table, (jnp.arange(top)[None, :] + turn) % top, axis=1)


def load_shares(count, total, bound, skew, full):
    weights = [(1 << 20) // math.isqrt(rank ** skew) + 1 for rank in range(1, count + 1)]
    largest = bound if full else min(bound, max(-(-total // count), total * weights[0] // sum(weights)))
    least = 1 if total - largest >= count - 1 else 0
    counts, surplus = [largest] + [least] * (count - 1), total - largest - least * (count - 1)
    while surplus > 0:
        movable = [i for i in range(1, count) if counts[i] < largest] or [i for i in range(1, count) if counts[i] < bound]
        whole, left = sum([weights[i] for i in movable]), surplus
        for i in movable:
            addition = min(bound - counts[i], max(1, left * weights[i] // whole), surplus)
            counts[i] = counts[i] + addition
            surplus = surplus - addition
    return np.array(counts)


def normal_values(rng, dims, deviation, most, cuts=(), held_as=jnp.bfloat16):
    values = jax.random.normal(rng, dims, jnp.float32) * deviation
    if len(cuts) > 0:
        values = level_of(rng, dims, cuts, -0.22, 0.18) * values
    return jnp.clip(values, min=-most, max=most).astype(held_as)


def setup_inputs(seed: int = 0) -> dict:
    streams_of = jax.random.split(jax.random.key(seed), 16)
    stream_in = normal_values(streams_of[0], (SEQUENCE_TOKENS, MODEL_WIDTH), 1.0, 6.0, ((0, 128),))
    query_rows = normal_values(streams_of[1], (SEQUENCE_TOKENS, MODEL_WIDTH), 1.0, 6.0, ((0, 64), (1, 2)))
    key_rows = normal_values(streams_of[2], (SEQUENCE_TOKENS, MODEL_WIDTH), 1.0, 6.0, ((0, 64), (1, 2)))
    value_rows = normal_values(streams_of[3], (SEQUENCE_TOKENS, MODEL_WIDTH), 1.0, 6.0, ((0, 64), (1, 2)))
    removal_key = normal_values(streams_of[4], (SEQUENCE_TOKENS, MODEL_WIDTH), 1.0, 6.0, ((0, 64), (1, 2)))
    learn_pre = draw_learn_pre(jax.random.fold_in(streams_of[15], 71), 0)
    log_rate = draw_log_rate(jax.random.fold_in(streams_of[15], 71), 0)
    norm_gain = jnp.clip(1.0 + 0.18 * jax.random.normal(streams_of[7], (MODEL_WIDTH,), jnp.float32), 0.099609375, 1.8984375).astype(jnp.bfloat16)
    out_weight = normal_values(streams_of[8], (MODEL_WIDTH, MODEL_WIDTH), MODEL_WIDTH ** -0.5, 0.125)
    ffn_gain = jnp.clip(1.0 + 0.18 * jax.random.normal(streams_of[9], (MODEL_WIDTH,), jnp.float32), 0.099609375, 1.8984375).astype(jnp.bfloat16)
    routes_keys = jax.random.split(jax.random.fold_in(streams_of[10], 1), SEQUENCE_TOKENS // HALF)
    routes_turns = jax.random.permutation(jax.random.fold_in(streams_of[10], 3), SEQUENCE_TOKENS // HALF)
    routes = jax.vmap(lambda own, number: deal_out(jax.random.fold_in(streams_of[10], 2), own, number, HALF, EXPERTS, TOPK, CAP, 1))(routes_keys, routes_turns).reshape((SEQUENCE_TOKENS, TOPK))
    route_weight = jnp.clip(0.1 + 0.9 * jax.random.uniform(streams_of[11], (SEQUENCE_TOKENS, TOPK), jnp.float32) ** level_of(streams_of[11], (SEQUENCE_TOKENS, TOPK), ((0, 128),), -0.2, 0.2), 0.1, 1.0)
    expert_gate = normal_values(streams_of[12], (2 * EXPERTS, MODEL_WIDTH, FFE // 2), MODEL_WIDTH ** -0.5, 0.125, ((0, 64), (2, 2)))
    expert_up = normal_values(streams_of[13], (2 * EXPERTS, MODEL_WIDTH, FFE // 2), MODEL_WIDTH ** -0.5, 0.125, ((0, 64), (2, 2)))
    expert_down = normal_values(streams_of[14], (2 * EXPERTS, FFE // 2, MODEL_WIDTH), FFE ** -0.5, 0.09375, ((0, 64), (1, 2)))
    return dict(stream_in=stream_in, query_rows=query_rows, key_rows=key_rows, value_rows=value_rows, removal_key=removal_key, learn_pre=learn_pre, log_rate=log_rate, norm_gain=norm_gain, out_weight=out_weight, ffn_gain=ffn_gain, routes=routes, route_weight=route_weight, expert_gate=expert_gate, expert_up=expert_up, expert_down=expert_down)


HIGH = lax.Precision.HIGHEST
GROUP_EPS = 0.00064
NORM_EPS = 1e-06
UNIT_EPS = 1e-06

def recurrence(carried, inputs):
    queries, key_vals, values, unit_key, pull_key, decays = inputs
    along_unit = jnp.einsum('hvk,hk->hv', carried, unit_key, precision=HIGH)
    carried = carried * decays[:, None, :] - along_unit[:, :, None] * pull_key[:, None, :] + values[:, :, None] * key_vals[:, None, :]
    return (carried, jnp.einsum('hvk,hk->hv', carried, queries, precision=HIGH))

def to_heads(array):
    return array.astype(jnp.float32).reshape(SEQUENCE_TOKENS, HEADS, HEAD)

def expert_rows(routed, gate_pair, up_pair, down_pair):
    quarter = FFE // 4
    running_sum = jnp.zeros((routed.shape[0], MODEL_WIDTH), jnp.float32)
    for half_index in range(2):
        for column_index in range(2):
            start_col = column_index * quarter
            gate_act = jnp.dot(routed, gate_pair[half_index, :, start_col:start_col + quarter], preferred_element_type=jnp.float32)
            up_act = jnp.dot(routed, up_pair[half_index, :, start_col:start_col + quarter], preferred_element_type=jnp.float32)
            hidden = (jax.nn.silu(gate_act) * up_act).astype(jnp.bfloat16)
            partial_out = jnp.dot(hidden, down_pair[half_index, start_col:start_col + quarter, :], preferred_element_type=jnp.float32).astype(jnp.bfloat16)
            running_sum = running_sum + partial_out.astype(jnp.float32)
    return running_sum.astype(jnp.bfloat16)

def reference(stream_in, query_rows, key_rows, value_rows, removal_key, learn_pre, log_rate, norm_gain, out_weight, ffn_gain, routes, route_weight, expert_gate, expert_up, expert_down):
    removal = to_heads(removal_key)
    unit_key = removal / jnp.sqrt(lax.optimization_barrier(jnp.sum(removal * removal, axis=-1, keepdims=True)) + UNIT_EPS)
    pull_key = unit_key * jax.nn.sigmoid(to_heads(learn_pre))
    decays = jnp.exp(-jnp.exp(to_heads(log_rate)))
    initial = jnp.zeros((HEADS, HEAD, HEAD), jnp.float32)
    inputs = (to_heads(query_rows), to_heads(key_rows), to_heads(value_rows), unit_key, pull_key, decays)
    _, mixed = lax.scan(recurrence, initial, inputs)
    centred = mixed - lax.optimization_barrier(jnp.mean(mixed, axis=-1, keepdims=True))
    variance = lax.optimization_barrier(jnp.mean(centred * centred, axis=-1, keepdims=True))
    normed = (centred * lax.rsqrt(variance + GROUP_EPS)).reshape(SEQUENCE_TOKENS, MODEL_WIDTH)
    normed = (normed * norm_gain.astype(jnp.float32)).astype(jnp.bfloat16)
    attended = stream_in.astype(jnp.float32) + jnp.dot(normed, out_weight, preferred_element_type=jnp.float32)
    scaling = lax.rsqrt(lax.optimization_barrier(jnp.mean(attended * attended, axis=-1, keepdims=True)) + NORM_EPS)
    ffn_in = (attended * scaling * ffn_gain.astype(jnp.float32)).astype(jnp.bfloat16)
    sources = SEQUENCE_TOKENS // HALF
    pairs = HALF * TOPK
    expert_ids = routes.reshape(sources, pairs).astype(jnp.int32)
    one_hot = (expert_ids[:, :, None] == jnp.arange(EXPERTS, dtype=jnp.int32)[None, None, :]).astype(jnp.int32)
    slot_index = (lax.optimization_barrier(jnp.sum(jnp.cumsum(one_hot, axis=1) * one_hot, axis=2)) - 1).astype(jnp.int32)
    source_index = jnp.broadcast_to(jnp.arange(sources, dtype=jnp.int32)[:, None], (sources, pairs))
    pair_rows = jnp.repeat(ffn_in.reshape(sources, HALF, MODEL_WIDTH), TOPK, axis=1)
    buffer = jnp.zeros((EXPERTS, sources, CAP, MODEL_WIDTH), jnp.bfloat16)
    buffer = buffer.at[expert_ids, source_index, slot_index].set(pair_rows)

    def run_expert(operands):
        routed, gate_pair, up_pair, down_pair = operands
        outcome = expert_rows(routed.reshape(sources * CAP, MODEL_WIDTH), gate_pair, up_pair, down_pair)
        return outcome.reshape(sources, CAP, MODEL_WIDTH)
    results = lax.map(run_expert, (buffer, expert_gate.reshape(EXPERTS, 2, MODEL_WIDTH, FFE // 2), expert_up.reshape(EXPERTS, 2, MODEL_WIDTH, FFE // 2), expert_down.reshape(EXPERTS, 2, FFE // 2, MODEL_WIDTH)))
    picked = results[expert_ids, source_index, slot_index].astype(jnp.float32)
    weights = route_weight.reshape(sources, pairs)
    mixture = lax.optimization_barrier(jnp.sum((picked * weights[:, :, None]).reshape(sources, HALF, TOPK, MODEL_WIDTH), axis=2))
    return (attended + mixture.reshape(SEQUENCE_TOKENS, MODEL_WIDTH)).astype(jnp.bfloat16)
```

```python
import functools
from typing import NamedTuple

import jax
import jax.numpy as jnp
from jax import lax
from jax.experimental import pallas as pl
from jax.experimental.pallas import tpu as pltpu
from jax.sharding import Mesh
from jax.sharding import PartitionSpec as P

HEAD = 64
LANES = 128
F32 = jnp.float32
BF16 = jnp.bfloat16
UNIT_EPS = 1e-06


def split(x):
    high = x.astype(BF16)
    return high, (x - high.astype(F32)).astype(BF16)


def mxu(x, y, dims=((1,), (0,))):
    return lax.dot_general(x, y, (dims, ((), ())), preferred_element_type=F32)


def packed(x):
    return jnp.concatenate(x, axis=1)


def spread(y):
    high, low = y
    top = jnp.concatenate((high, low), axis=1)
    return jnp.concatenate((top, top), axis=0)


def folded(z):
    half = z.shape[1] // 2
    return z[:, :half] + z[:, half:]


def product(x, y):
    return folded(mxu(packed(x), spread(y)))


def iota(shape, dim):
    return lax.broadcasted_iota(jnp.int32, shape, dim)


class Masks(NamedTuple):
    same_head: jax.Array
    lower: jax.Array


class Prepared(NamedTuple):
    left: list
    right: list
    values: jax.Array
    starts: jax.Array
    query_now: jax.Array
    pull_tail: jax.Array
    key_tail: jax.Array
    decay_all: jax.Array


def mixer_prepare(refs, lanes, masks):
    q_ref, k_ref, v_ref, r_ref, l_ref, g_ref = refs
    tokens = q_ref.shape[0]
    removal = r_ref[:, lanes].astype(F32)
    squares = split(removal * removal)
    total = mxu(packed(squares), jnp.concatenate((masks.same_head, masks.same_head), axis=0))
    unit = removal * lax.rsqrt(total + UNIT_EPS)
    pull = unit * jax.nn.sigmoid(l_ref[:, lanes].astype(F32))
    log_decay = -jnp.exp(g_ref[:, lanes])
    high = log_decay.astype(BF16)
    rest = log_decay - high.astype(F32)
    mid = rest.astype(BF16)
    low = (rest - mid.astype(F32)).astype(BF16)
    stacked = jnp.concatenate((packed((high, mid)), packed((low, jnp.zeros_like(low)))), axis=0)
    cumul = folded(mxu(packed((masks.lower, masks.lower)), stacked))
    middle = cumul[tokens // 2 - 1 : tokens // 2]
    end = cumul[tokens - 1 : tokens]
    grown = jnp.exp(middle - cumul)
    faded = jnp.exp(cumul - middle)
    unit_hat = unit * jnp.exp(cumul - log_decay - middle)
    query_hat = q_ref[:, lanes].astype(F32) * faded
    pull_hat = pull * grown
    key_hat = k_ref[:, lanes].astype(F32) * grown
    from_start = jnp.exp(middle)
    to_end = jnp.exp(end - middle)
    values = v_ref[:, lanes]
    left = [jnp.concatenate(p, axis=0) for p in zip(split(unit_hat), split(query_hat))]
    right = [jnp.concatenate(p, axis=0) for p in zip(split(pull_hat), split(key_hat))]
    return Prepared(
        left,
        right,
        jnp.concatenate((values, values), axis=0),
        pltpu.roll(unit_hat * from_start, HEAD, 1),
        query_hat * from_start,
        spread(split(pull_hat * to_end)),
        jnp.concatenate(split(key_hat * to_end), axis=0),
        jnp.exp(end),
    )


def mixer_kernel(pairs, q_ref, k_ref, v_ref, r_ref, l_ref, g_ref, z_ref, local_ref, carry_ref):
    refs = (q_ref, k_ref, v_ref, r_ref, l_ref, g_ref)
    tokens = q_ref.shape[0]
    row, col = iota((tokens, tokens), 0), iota((tokens, tokens), 1)
    strict, upto, apart = row > col, row >= col, row ^ col
    first = iota((tokens, LANES), 1) < HEAD
    masks = Masks(
        ((iota((LANES, LANES), 0) < HEAD) == (iota((LANES, LANES), 1) < HEAD)).astype(BF16),
        upto.astype(BF16),
    )
    own_lanes = (first, jnp.logical_not(first))
    lanes = [slice(pair * LANES, (pair + 1) * LANES) for pair in range(pairs)]
    ready = [mixer_prepare(refs, part, masks) for part in lanes]
    heads = [(pair, head) for pair in range(pairs) for head in range(2)]

    scores = []
    for pair, head in heads:
        inside = jnp.concatenate((own_lanes[head], own_lanes[head]), axis=0)
        own = [jnp.where(inside, x, jnp.zeros_like(x)) for x in ready[pair].left]
        right = ready[pair].right
        scores.append(
            mxu(packed(own), packed((right[0], right[0])), ((1,), (1,)))
            + mxu(own[0], right[1], ((1,), (1,)))
        )
    mix_pull = [jnp.where(strict, s[:tokens, :tokens], 0.0) for s in scores]
    mix_key = [jnp.where(strict, s[:tokens, tokens:], 0.0) for s in scores]
    read_pull = [split(jnp.where(upto, s[tokens:, :tokens], 0.0)) for s in scores]
    read_key = [jnp.where(upto, s[tokens:, tokens:], 0.0) for s in scores]
    by_key = []
    for n, (pair, head) in enumerate(heads):
        both = [jnp.concatenate(p, axis=0) for p in zip(split(mix_key[n]), split(read_key[n]))]
        by_key.append(mxu(packed(both), ready[pair].values))

    identity = (row == col).astype(F32)
    inverse = [identity - jnp.where(apart < 2, m, 0.0) for m in mix_pull]
    size = 2
    while size < tokens:
        within = (apart >= size) & (apart < 2 * size)
        parts = [split(x) for x in inverse]
        edges = [split(jnp.where(within, m, 0.0)) for m in mix_pull]
        steps = [split(product(x, y)) for x, y in zip(parts, edges)]
        inverse = [x - product(y, z) for x, y, z in zip(inverse, steps, parts)]
        size *= 2

    answers, solved, outer = [], [], []
    for n, (pair, head) in enumerate(heads):
        sources = jnp.where(own_lanes[head], by_key[n][:tokens], ready[pair].starts)
        answers.append(split(product(split(inverse[n]), split(sources))))
    for n, (pair, head) in enumerate(heads):
        solved.append(product(read_pull[n], answers[n]))
        stacked = jnp.concatenate(answers[n], axis=0)
        outer.append(folded(mxu(stacked, ready[pair].pull_tail, ((0,), (0,)))))

    half = iota((HEAD, LANES), 1) < HEAD
    diagonal = (iota((HEAD, LANES), 1) % HEAD) == iota((HEAD, LANES), 0)
    for pair in range(pairs):
        one, two = 2 * pair, 2 * pair + 1
        local_ref[:, lanes[pair]] = jnp.where(
            first, by_key[one][tokens:] - solved[one], by_key[two][tokens:] - solved[two]
        )
        carry_ref[:, lanes[pair]] = ready[pair].query_now - pltpu.roll(
            jnp.where(first, solved[two], solved[one]), HEAD, 1
        )
        written = mxu(ready[pair].values, ready[pair].key_tail, ((0,), (0,)))
        z_ref[pair, :HEAD] = jnp.where(
            half, written[:HEAD] - outer[one][:HEAD], written[HEAD:] - outer[two][HEAD:]
        )
        z_ref[pair, HEAD:] = jnp.where(diagonal, ready[pair].decay_all, 0.0) - jnp.where(
            half, outer[one][HEAD:], outer[two][:HEAD]
        )


def mixer_blocks(queries, keys, values, removal, learn, rates, per_step=2):
    tokens, width = queries.shape
    pairs = width // LANES
    rows = pl.BlockSpec((tokens, per_step * LANES), lambda i: (0, i))
    return pl.pallas_call(
        functools.partial(mixer_kernel, per_step),
        grid=(pairs // per_step,),
        in_specs=[rows] * 6,
        out_specs=[pl.BlockSpec((per_step, 2 * HEAD, LANES), lambda i: (i, 0, 0)), rows, rows],
        out_shape=[
            jax.ShapeDtypeStruct((pairs, 2 * HEAD, LANES), F32),
            jax.ShapeDtypeStruct((tokens, width), F32),
            jax.ShapeDtypeStruct((tokens, width), F32),
        ],
        name="mixer_blocks",
    )(queries, keys, values, removal, learn, rates)


MESH = pl.DeviceIdType.MESH
GROUP_EPS = 0.00064
NORM_EPS = 1e-06
COLUMNS = 512


def block_diagonal(rows):
    first = iota(rows.shape, 1) < HEAD
    zero = jnp.zeros_like(rows)
    return jnp.concatenate((jnp.where(first, rows, zero), jnp.where(first, zero, rows)), axis=0)


def mapped(earlier, later):
    return product(split(earlier), split(block_diagonal(later[HEAD:])))


def compose(earlier, later):
    joined = mapped(earlier, later)
    return jnp.concatenate((joined[:HEAD] + later[:HEAD], joined[HEAD:]), axis=0)


def prefixes(blocks):
    done, step = list(blocks), 1
    while step < len(done):
        for j in range(len(done)):
            if (j // step) % 2 == 1:
                done[j] = compose(done[j // step * step - 1], done[j])
        step *= 2
    return done


def joined_all(blocks):
    while len(blocks) > 1:
        pairs = [compose(*blocks[j : j + 2]) for j in range(0, len(blocks) - 1, 2)]
        blocks = pairs + (blocks[-1:] if len(blocks) % 2 else [])
    return blocks[0]


def remote(source, target, sends, receives, place):
    return pltpu.make_async_remote_copy(
        src_ref=source,
        dst_ref=target,
        send_sem=sends,
        recv_sem=receives,
        device_id=place,
        device_id_type=MESH,
    )


def entering_states(z_ref, by_member, by_group, total_ref, found, entered, sems):
    group, member, core = (lax.axis_index(a) for a in ("grp", "mem", "tp"))
    members, groups = by_member.shape[0], by_group.shape[0]
    sent_1, got_1, sent_2, got_2, sent_3, got_3 = sems

    first = []
    for offset in range(1, members):
        peer = lax.rem(member + offset, members)
        copy = remote(
            z_ref.at[peer],
            by_member.at[member],
            sent_1.at[offset],
            got_1.at[member],
            (group, peer, core),
        )
        copy.start()
        first.append(copy)
    by_member[member] = z_ref[member]
    for offset in range(1, members):
        peer = lax.rem(member + offset, members)
        remote(
            z_ref.at[peer], by_member.at[peer], sent_1.at[offset], got_1.at[peer], (group, peer, core)
        ).wait_recv()
    inclusive = prefixes([by_member[j] for j in range(members)])
    total_ref[...] = inclusive[-1]

    second = []
    for offset in range(1, groups):
        peer = lax.rem(group + offset, groups)
        copy = remote(
            total_ref,
            by_group.at[group],
            sent_2.at[offset],
            got_2.at[group],
            (peer, member, core),
        )
        copy.start()
        second.append(copy)
    maps = [spread(split(block_diagonal(inclusive[j][HEAD:]))) for j in range(members - 1)]
    by_group[group] = total_ref[...]
    for offset in range(1, groups):
        peer = lax.rem(group + offset, groups)
        remote(
            total_ref, by_group.at[peer], sent_2.at[offset], got_2.at[peer], (peer, member, core)
        ).wait_recv()
    shape = total_ref.shape
    neutral = ((iota(shape, 1) % HEAD) + HEAD == iota(shape, 0)).astype(F32)
    before = [jnp.where(j < group, by_group[j], neutral) for j in range(groups - 1)]
    start = joined_all(before)[:HEAD]
    parts = packed(split(start))
    found[0] = start
    for j in range(1, members):
        found[j] = folded(mxu(parts, maps[j - 1])) + inclusive[j - 1][:HEAD]

    third = []
    for offset in range(1, members):
        peer = lax.rem(member + offset, members)
        copy = remote(
            found.at[peer],
            entered.at[member],
            sent_3.at[offset],
            got_3.at[member],
            (group, peer, core),
        )
        copy.start()
        third.append(copy)
    entered[member] = found[member]
    for offset in range(1, members):
        peer = lax.rem(member + offset, members)
        remote(
            found.at[peer], entered.at[peer], sent_3.at[offset], got_3.at[peer], (group, peer, core)
        ).wait_recv()
    return first + second + third


def normed_heads(local_ref, carry_ref, entered, gain_ref, normed):
    same_head = ((iota((LANES, LANES), 0) < HEAD) == (iota((LANES, LANES), 1) < HEAD)).astype(BF16)
    same_head = jnp.concatenate((same_head, same_head), axis=0)
    pairs = entered.shape[0]
    lanes = [slice(pair * LANES, (pair + 1) * LANES) for pair in range(pairs)]
    mixed = []
    for pair in range(pairs):
        high, low = split(block_diagonal(entered[pair]))
        rhs = jnp.concatenate((packed((high, high)), packed((low, low))), axis=0)
        read = folded(mxu(packed(split(carry_ref[:, lanes[pair]])), rhs, ((1,), (1,))))
        mixed.append(local_ref[:, lanes[pair]] + read)
    centred = [x - mxu(packed(split(x)), same_head) * (1.0 / HEAD) for x in mixed]
    variance = [mxu(packed(split(x * x)), same_head) * (1.0 / HEAD) for x in centred]
    for pair in range(pairs):
        scaled = centred[pair] * lax.rsqrt(variance[pair] + GROUP_EPS)
        normed[:, lanes[pair]] = (scaled * gain_ref[:, lanes[pair]].astype(F32)).astype(BF16)


def slot_map(routes_ref, experts, capacity):
    half = routes_ref.shape[0]
    shape = (half, experts * capacity)
    lane = iota(shape, 1)
    expert, slot = lane // capacity, lane % capacity
    named = [routes_ref[:, k : k + 1] == expert for k in range(2)]
    chosen = (named[0] | named[1]).astype(F32)
    earlier = (iota((half, half), 0) > iota((half, half), 1)).astype(BF16)
    place = mxu(earlier, chosen.astype(BF16))
    kept = jnp.where(place == slot.astype(F32), chosen, 0.0)
    return kept, named


def mixer_finish_kernel(
    experts,
    z_ref,
    local_ref,
    carry_ref,
    gain_ref,
    stream_ref,
    weight_ref,
    ffn_gain_ref,
    routes_ref,
    attended_ref,
    dispatched_ref,
    by_member,
    by_group,
    total_ref,
    found,
    entered,
    normed,
    weight,
    partial,
    other,
    weight_sem,
    sent_4,
    got_4,
    *sems,
):
    group, member, core = (lax.axis_index(a) for a in ("grp", "mem", "tp"))
    members, groups = by_member.shape[0], by_group.shape[0]
    barrier = pltpu.get_barrier_semaphore()
    peers = [(group, lax.rem(member + o, members), core) for o in range(1, members)]
    peers += [(lax.rem(group + o, groups), member, core) for o in range(1, groups)]
    peers += [(group, member, 1 - core)]
    for peer in peers:
        pl.semaphore_signal(barrier, inc=1, device_id=peer, device_id_type=MESH)
    depth = weight.shape[0]
    fetch = pltpu.make_async_copy(weight_ref.at[pl.ds(core * depth, depth)], weight, weight_sem)
    fetch.start()
    pl.semaphore_wait(barrier, len(peers))

    copies = entering_states(z_ref, by_member, by_group, total_ref, found, entered, sems)
    normed_heads(local_ref, carry_ref, entered, gain_ref, normed)
    fetch.wait()
    half = stream_ref.shape[0]
    chunks = partial.shape[0]
    mine, theirs = pl.ds(core * half, half), pl.ds((1 - core) * half, half)
    for n in range(chunks):
        partial[n] = jnp.dot(
            normed[...], weight[:, n * COLUMNS : (n + 1) * COLUMNS], preferred_element_type=F32
        )
        copy = remote(
            partial.at[n, theirs],
            other.at[n],
            sent_4.at[n],
            got_4.at[n],
            (group, member, 1 - core),
        )
        copy.start()
        copies.append(copy)
    kept, _ = slot_map(routes_ref, experts, dispatched_ref.shape[0] // experts)
    kept = kept.astype(BF16)
    squares = jnp.zeros((half, 1), F32)
    for n in range(chunks):
        lanes = slice(n * COLUMNS, (n + 1) * COLUMNS)
        copies[n - chunks].wait_recv()
        attended = stream_ref[:, lanes].astype(F32) + (partial[n, mine] + other[n])
        attended_ref[:, lanes] = attended
        squares = squares + jnp.sum(attended * attended, axis=1, keepdims=True)
    width = chunks * COLUMNS
    scaling = lax.rsqrt(squares * (1.0 / width) + NORM_EPS)
    for n in range(chunks):
        lanes = slice(n * COLUMNS, (n + 1) * COLUMNS)
        ffn_in = attended_ref[:, lanes] * scaling * ffn_gain_ref[:, lanes].astype(F32)
        dispatched_ref[:, lanes] = mxu(kept, ffn_in.astype(BF16), ((0,), (0,))).astype(BF16)
    for copy in copies:
        copy.wait_send()


def mixer_finish(z, local_read, carry_read, gain, stream, weight, ffn_gain, routes, experts, capacity):
    half, width = stream.shape
    tokens = local_read.shape[0]
    members, groups = lax.axis_size("mem"), lax.axis_size("grp")
    chunks = width // COLUMNS
    vmem = pl.BlockSpec(memory_space=pltpu.VMEM)
    dma = pltpu.SemaphoreType.DMA
    return pl.pallas_call(
        functools.partial(mixer_finish_kernel, experts),
        in_specs=[vmem] * 5 + [pl.BlockSpec(memory_space=pl.ANY)] + [vmem] * 2,
        out_specs=[vmem, vmem],
        out_shape=[
            jax.ShapeDtypeStruct((half, width), F32),
            jax.ShapeDtypeStruct((experts * capacity, width), BF16),
        ],
        scratch_shapes=[
            pltpu.VMEM((members, 2 * HEAD, LANES), F32),
            pltpu.VMEM((groups, 2 * HEAD, LANES), F32),
            pltpu.VMEM((2 * HEAD, LANES), F32),
            pltpu.VMEM((members, HEAD, LANES), F32),
            pltpu.VMEM((members, HEAD, LANES), F32),
            pltpu.VMEM((tokens, width // 2), BF16),
            pltpu.VMEM((width // 2, width), BF16),
            pltpu.VMEM((chunks, tokens, COLUMNS), F32),
            pltpu.VMEM((chunks, half, COLUMNS), F32),
            dma,
            dma((chunks,)),
            dma((chunks,)),
            dma((members,)),
            dma((members,)),
            dma((groups,)),
            dma((groups,)),
            dma((members,)),
            dma((members,)),
        ],
        compiler_params=pltpu.CompilerParams(
            collective_id=0, has_side_effects=True, vmem_limit_bytes=48 * 1024 * 1024
        ),
        name="mixer_finish",
    )(z, local_read, carry_read, gain, stream, weight, ffn_gain, routes)


TOPK = 2
SP_TP = ("grp", "mem", "tp")
SP = ("grp", "mem")


def from_partner(array, axis, bit):
    return lax.ppermute(array, axis, [(i, i ^ 1 << bit) for i in range(lax.axis_size(axis))])


def split_up(array, dim, length):
    before, after = (array.shape[:dim], array.shape[dim + 1 :])
    return jnp.moveaxis(array.reshape(*before, length, -1, *after), dim, 0)


def sent_and_summed(array, axis, dim):
    length = lax.axis_size(axis)
    pieces = lax.all_to_all(split_up(array, dim, length), axis, 0, 0, tiled=True)
    return jnp.sum(pieces.astype(jnp.float32), axis=0)


def local(
    stream_in,
    query_rows,
    key_rows,
    value_rows,
    removal_key,
    learn_pre,
    log_rate,
    norm_gain,
    out_weight,
    ffn_gain,
    routes,
    route_weight,
    expert_gate,
    expert_up,
    expert_down,
):
    half_rows, width = stream_in.shape
    experts = lax.axis_size(SP) // 2
    peers = lax.axis_size(SP_TP)
    capacity = 2 * TOPK * half_rows // experts
    z, local_read, carry_read = mixer_blocks(
        query_rows, key_rows, value_rows, removal_key, learn_pre, log_rate, per_step=4
    )
    attended, dispatched = mixer_finish(
        z,
        local_read,
        carry_read,
        norm_gain.reshape(1, -1),
        stream_in,
        out_weight,
        ffn_gain.reshape(1, -1),
        routes,
        experts,
        capacity,
    )
    copies = jnp.broadcast_to(
        dispatched.reshape(experts, 1, capacity, width), (experts, 4, capacity, width)
    )
    routed = lax.all_to_all(
        copies.reshape(peers * capacity, width), SP_TP, split_axis=0, concat_axis=0, tiled=True
    )
    gate_act = jnp.dot(routed, expert_gate[0], preferred_element_type=jnp.float32)
    up_act = jnp.dot(routed, expert_up[0], preferred_element_type=jnp.float32)
    hidden = (jax.nn.silu(gate_act) * up_act).astype(jnp.bfloat16)
    partial_out = jnp.dot(hidden, expert_down[0], preferred_element_type=jnp.float32).astype(
        jnp.bfloat16
    )
    partial_out = partial_out.reshape(peers, capacity, width)
    pair_bit = lax.axis_index(SP) % 2
    half_width = width // 2
    kept_half = lax.dynamic_slice_in_dim(partial_out, pair_bit * half_width, half_width, 2)
    sent_half = lax.dynamic_slice_in_dim(partial_out, (1 - pair_bit) * half_width, half_width, 2)
    partner_half = from_partner(sent_half, SP, 0)
    pair_sum = kept_half.astype(jnp.float32) + partner_half.astype(jnp.float32)
    expert_out = sent_and_summed(pair_sum.astype(jnp.bfloat16), "tp", 2).astype(jnp.bfloat16)
    returned = lax.all_to_all(expert_out, SP_TP, split_axis=0, concat_axis=2, tiled=True)
    returned = returned.reshape(capacity, experts, width)
    lane = jnp.arange(experts, dtype=jnp.int32)
    one_hot = (routes[:, :, None] == lane).any(axis=1)
    earlier = jnp.arange(half_rows)[:, None] > jnp.arange(half_rows)[None, :]
    place = jnp.dot(earlier.astype(jnp.float32), one_hot.astype(jnp.float32))
    slot = jnp.take_along_axis(place.astype(jnp.int32), routes, axis=1).reshape(-1)
    back_index = slot * experts + routes.reshape(-1)
    back_map = (
        back_index[:, None] == jnp.arange(capacity * experts, dtype=jnp.int32)[None, :]
    ).astype(jnp.bfloat16)
    picked = jnp.dot(
        back_map, returned.reshape(capacity * experts, width), preferred_element_type=jnp.float32
    ).reshape(half_rows, TOPK, width)
    mixture = jnp.sum(picked * route_weight[:, :, None], axis=1)
    return (attended + mixture).astype(jnp.bfloat16)


def solution(mesh):
    sp = mesh.shape["sp"]
    groups = 1
    while groups * groups < sp:
        groups *= 2
    torus = Mesh(
        mesh.devices.reshape(sp // groups, groups, mesh.shape["tp"]), ("grp", "mem", "tp")
    )
    return jax.shard_map(
        local,
        mesh=torus,
        in_specs=(
            P(SP_TP, None),
            P(SP, "tp"),
            P(SP, "tp"),
            P(SP, "tp"),
            P(SP, "tp"),
            P(SP, "tp"),
            P(SP, "tp"),
            P("tp"),
            P(),
            P(),
            P(SP_TP, None),
            P(SP_TP, None),
            P(SP, None, "tp"),
            P(SP, None, "tp"),
            P(SP, "tp", None),
        ),
        out_specs=P(SP_TP, None),
        check_vma=False,
    )
```

```python
import functools
import math
from typing import NamedTuple

import jax
import jax.numpy as jnp
from jax import lax
from jax.experimental import pallas as pl
from jax.experimental.pallas import tpu as pltpu
from jax.sharding import Mesh
from jax.sharding import PartitionSpec as P

HEAD = 64
LANES = 128
F32 = jnp.float32
BF16 = jnp.bfloat16
UNIT_EPS = 1e-06


def split(x):
    high = x.astype(BF16)
    return high, (x - high.astype(F32)).astype(BF16)


def mxu(x, y, dims=((1,), (0,))):
    return lax.dot_general(x, y, (dims, ((), ())), preferred_element_type=F32)


def packed(x):
    return jnp.concatenate(x, axis=1)


def spread(y):
    high, low = y
    top = jnp.concatenate((high, low), axis=1)
    return jnp.concatenate((top, top), axis=0)


def folded(z):
    half = z.shape[1] // 2
    return z[:, :half] + z[:, half:]


def product(x, y):
    return folded(mxu(packed(x), spread(y)))


def iota(shape, dim):
    return lax.broadcasted_iota(jnp.int32, shape, dim)


class Masks(NamedTuple):
    same_head: jax.Array
    lower: jax.Array


class Prepared(NamedTuple):
    left: list
    right: list
    values: jax.Array
    starts: jax.Array
    query_now: jax.Array
    pull_tail: jax.Array
    key_tail: jax.Array
    decay_all: jax.Array


def mixer_prepare(refs, lanes, masks):
    q_ref, k_ref, v_ref, r_ref, l_ref, g_ref = refs
    tokens = q_ref.shape[0]
    removal = r_ref[:, lanes].astype(F32)
    squares = split(removal * removal)
    total = mxu(packed(squares), jnp.concatenate((masks.same_head, masks.same_head), axis=0))
    unit = removal * lax.rsqrt(total + UNIT_EPS)
    pull = unit * jax.nn.sigmoid(l_ref[:, lanes].astype(F32))
    log_decay = -jnp.exp(g_ref[:, lanes])
    high = log_decay.astype(BF16)
    rest = log_decay - high.astype(F32)
    mid = rest.astype(BF16)
    low = (rest - mid.astype(F32)).astype(BF16)
    stacked = jnp.concatenate((packed((high, mid)), packed((low, jnp.zeros_like(low)))), axis=0)
    cumul = folded(mxu(packed((masks.lower, masks.lower)), stacked))
    middle = cumul[tokens // 2 - 1 : tokens // 2]
    end = cumul[tokens - 1 : tokens]
    grown = jnp.exp(middle - cumul)
    faded = jnp.exp(cumul - middle)
    unit_hat = unit * jnp.exp(cumul - log_decay - middle)
    query_hat = q_ref[:, lanes].astype(F32) * faded
    pull_hat = pull * grown
    key_hat = k_ref[:, lanes].astype(F32) * grown
    from_start = jnp.exp(middle)
    to_end = jnp.exp(end - middle)
    values = v_ref[:, lanes]
    left = [jnp.concatenate(p, axis=0) for p in zip(split(unit_hat), split(query_hat))]
    right = [jnp.concatenate(p, axis=0) for p in zip(split(pull_hat), split(key_hat))]
    return Prepared(
        left,
        right,
        jnp.concatenate((values, values), axis=0),
        pltpu.roll(unit_hat * from_start, HEAD, 1),
        query_hat * from_start,
        spread(split(pull_hat * to_end)),
        jnp.concatenate(split(key_hat * to_end), axis=0),
        jnp.exp(end),
    )


def mixer_kernel(pairs, q_ref, k_ref, v_ref, r_ref, l_ref, g_ref, z_ref, local_ref, carry_ref):
    refs = (q_ref, k_ref, v_ref, r_ref, l_ref, g_ref)
    tokens = q_ref.shape[0]
    row, col = iota((tokens, tokens), 0), iota((tokens, tokens), 1)
    strict, upto, apart = row > col, row >= col, row ^ col
    first = iota((tokens, LANES), 1) < HEAD
    masks = Masks(
        ((iota((LANES, LANES), 0) < HEAD) == (iota((LANES, LANES), 1) < HEAD)).astype(BF16),
        upto.astype(BF16),
    )
    own_lanes = (first, jnp.logical_not(first))
    lanes = [slice(pair * LANES, (pair + 1) * LANES) for pair in range(pairs)]
    ready = [mixer_prepare(refs, part, masks) for part in lanes]
    heads = [(pair, head) for pair in range(pairs) for head in range(2)]

    scores = []
    for pair, head in heads:
        inside = jnp.concatenate((own_lanes[head], own_lanes[head]), axis=0)
        own = [jnp.where(inside, x, jnp.zeros_like(x)) for x in ready[pair].left]
        right = ready[pair].right
        scores.append(
            mxu(packed(own), packed((right[0], right[0])), ((1,), (1,)))
            + mxu(own[0], right[1], ((1,), (1,)))
        )
    mix_pull = [jnp.where(strict, s[:tokens, :tokens], 0.0) for s in scores]
    mix_key = [jnp.where(strict, s[:tokens, tokens:], 0.0) for s in scores]
    read_pull = [split(jnp.where(upto, s[tokens:, :tokens], 0.0)) for s in scores]
    read_key = [jnp.where(upto, s[tokens:, tokens:], 0.0) for s in scores]
    by_key = []
    for n, (pair, head) in enumerate(heads):
        both = [jnp.concatenate(p, axis=0) for p in zip(split(mix_key[n]), split(read_key[n]))]
        by_key.append(mxu(packed(both), ready[pair].values))

    identity = (row == col).astype(F32)
    inverse = [identity - jnp.where(apart < 2, m, 0.0) for m in mix_pull]
    size = 2
    while size < tokens:
        within = (apart >= size) & (apart < 2 * size)
        parts = [split(x) for x in inverse]
        edges = [split(jnp.where(within, m, 0.0)) for m in mix_pull]
        steps = [split(product(x, y)) for x, y in zip(parts, edges)]
        inverse = [x - product(y, z) for x, y, z in zip(inverse, steps, parts)]
        size *= 2

    answers, solved, outer = [], [], []
    for n, (pair, head) in enumerate(heads):
        sources = jnp.where(own_lanes[head], by_key[n][:tokens], ready[pair].starts)
        answers.append(split(product(split(inverse[n]), split(sources))))
    for n, (pair, head) in enumerate(heads):
        solved.append(product(read_pull[n], answers[n]))
        stacked = jnp.concatenate(answers[n], axis=0)
        outer.append(folded(mxu(stacked, ready[pair].pull_tail, ((0,), (0,)))))

    half = iota((HEAD, LANES), 1) < HEAD
    diagonal = (iota((HEAD, LANES), 1) % HEAD) == iota((HEAD, LANES), 0)
    for pair in range(pairs):
        one, two = 2 * pair, 2 * pair + 1
        local_ref[:, lanes[pair]] = jnp.where(
            first, by_key[one][tokens:] - solved[one], by_key[two][tokens:] - solved[two]
        )
        carry_ref[:, lanes[pair]] = ready[pair].query_now - pltpu.roll(
            jnp.where(first, solved[two], solved[one]), HEAD, 1
        )
        written = mxu(ready[pair].values, ready[pair].key_tail, ((0,), (0,)))
        z_ref[pair, :HEAD] = jnp.where(
            half, written[:HEAD] - outer[one][:HEAD], written[HEAD:] - outer[two][HEAD:]
        )
        z_ref[pair, HEAD:] = jnp.where(diagonal, ready[pair].decay_all, 0.0) - jnp.where(
            half, outer[one][HEAD:], outer[two][:HEAD]
        )


def mixer_blocks(queries, keys, values, removal, learn, rates, per_step=2):
    tokens, width = queries.shape
    pairs = width // LANES
    rows = pl.BlockSpec((tokens, per_step * LANES), lambda i: (0, i))
    return pl.pallas_call(
        functools.partial(mixer_kernel, per_step),
        grid=(pairs // per_step,),
        in_specs=[rows] * 6,
        out_specs=[pl.BlockSpec((per_step, 2 * HEAD, LANES), lambda i: (i, 0, 0)), rows, rows],
        out_shape=[
            jax.ShapeDtypeStruct((pairs, 2 * HEAD, LANES), F32),
            jax.ShapeDtypeStruct((tokens, width), F32),
            jax.ShapeDtypeStruct((tokens, width), F32),
        ],
        name="mixer_blocks",
    )(queries, keys, values, removal, learn, rates)


MESH = pl.DeviceIdType.MESH
GROUP_EPS = 0.00064
NORM_EPS = 1e-06
COLUMNS = 512


def block_diagonal(rows):
    first = iota(rows.shape, 1) < HEAD
    zero = jnp.zeros_like(rows)
    return jnp.concatenate((jnp.where(first, rows, zero), jnp.where(first, zero, rows)), axis=0)


def mapped(earlier, later):
    return product(split(earlier), split(block_diagonal(later[HEAD:])))


def compose(earlier, later):
    joined = mapped(earlier, later)
    return jnp.concatenate((joined[:HEAD] + later[:HEAD], joined[HEAD:]), axis=0)


def prefixes(blocks):
    done, step = list(blocks), 1
    while step < len(done):
        for j in range(len(done)):
            if (j // step) % 2 == 1:
                done[j] = compose(done[j // step * step - 1], done[j])
        step *= 2
    return done


def joined_all(blocks):
    while len(blocks) > 1:
        pairs = [compose(*blocks[j : j + 2]) for j in range(0, len(blocks) - 1, 2)]
        blocks = pairs + (blocks[-1:] if len(blocks) % 2 else [])
    return blocks[0]


def remote(source, target, sends, receives, place):
    return pltpu.make_async_remote_copy(
        src_ref=source,
        dst_ref=target,
        send_sem=sends,
        recv_sem=receives,
        device_id=place,
        device_id_type=MESH,
    )


def entering_states(z_ref, by_member, by_group, total_ref, found, entered, sems):
    group, member, core = (lax.axis_index(a) for a in ("grp", "mem", "tp"))
    members, groups = by_member.shape[0], by_group.shape[0]
    sent_1, got_1, sent_2, got_2, sent_3, got_3 = sems

    first = []
    for offset in range(1, members):
        peer = lax.rem(member + offset, members)
        copy = remote(
            z_ref.at[peer],
            by_member.at[member],
            sent_1.at[offset],
            got_1.at[member],
            (group, peer, core),
        )
        copy.start()
        first.append(copy)
    by_member[member] = z_ref[member]
    for offset in range(1, members):
        peer = lax.rem(member + offset, members)
        remote(
            z_ref.at[peer], by_member.at[peer], sent_1.at[offset], got_1.at[peer], (group, peer, core)
        ).wait_recv()
    inclusive = prefixes([by_member[j] for j in range(members)])
    total_ref[...] = inclusive[-1]

    second = []
    for offset in range(1, groups):
        peer = lax.rem(group + offset, groups)
        copy = remote(
            total_ref,
            by_group.at[group],
            sent_2.at[offset],
            got_2.at[group],
            (peer, member, core),
        )
        copy.start()
        second.append(copy)
    maps = [spread(split(block_diagonal(inclusive[j][HEAD:]))) for j in range(members - 1)]
    by_group[group] = total_ref[...]
    for offset in range(1, groups):
        peer = lax.rem(group + offset, groups)
        remote(
            total_ref, by_group.at[peer], sent_2.at[offset], got_2.at[peer], (peer, member, core)
        ).wait_recv()
    shape = total_ref.shape
    neutral = ((iota(shape, 1) % HEAD) + HEAD == iota(shape, 0)).astype(F32)
    before = [jnp.where(j < group, by_group[j], neutral) for j in range(groups - 1)]
    start = joined_all(before)[:HEAD]
    parts = packed(split(start))
    found[0] = start
    for j in range(1, members):
        found[j] = folded(mxu(parts, maps[j - 1])) + inclusive[j - 1][:HEAD]

    third = []
    for offset in range(1, members):
        peer = lax.rem(member + offset, members)
        copy = remote(
            found.at[peer],
            entered.at[member],
            sent_3.at[offset],
            got_3.at[member],
            (group, peer, core),
        )
        copy.start()
        third.append(copy)
    entered[member] = found[member]
    for offset in range(1, members):
        peer = lax.rem(member + offset, members)
        remote(
            found.at[peer], entered.at[peer], sent_3.at[offset], got_3.at[peer], (group, peer, core)
        ).wait_recv()
    return first + second + third


def normed_heads(local_ref, carry_ref, entered, gain_ref, normed):
    same_head = ((iota((LANES, LANES), 0) < HEAD) == (iota((LANES, LANES), 1) < HEAD)).astype(BF16)
    same_head = jnp.concatenate((same_head, same_head), axis=0)
    pairs = entered.shape[0]
    lanes = [slice(pair * LANES, (pair + 1) * LANES) for pair in range(pairs)]
    mixed = []
    for pair in range(pairs):
        high, low = split(block_diagonal(entered[pair]))
        rhs = jnp.concatenate((packed((high, high)), packed((low, low))), axis=0)
        read = folded(mxu(packed(split(carry_ref[:, lanes[pair]])), rhs, ((1,), (1,))))
        mixed.append(local_ref[:, lanes[pair]] + read)
    centred = [x - mxu(packed(split(x)), same_head) * (1.0 / HEAD) for x in mixed]
    variance = [mxu(packed(split(x * x)), same_head) * (1.0 / HEAD) for x in centred]
    for pair in range(pairs):
        scaled = centred[pair] * lax.rsqrt(variance[pair] + GROUP_EPS)
        normed[:, lanes[pair]] = (scaled * gain_ref[:, lanes[pair]].astype(F32)).astype(BF16)


def slot_map(routes_ref, experts, capacity):
    half = routes_ref.shape[0]
    shape = (half, experts * capacity)
    lane = iota(shape, 1)
    expert, slot = lane // capacity, lane % capacity
    named = [routes_ref[:, k : k + 1] == expert for k in range(2)]
    chosen = (named[0] | named[1]).astype(F32)
    earlier = (iota((half, half), 0) > iota((half, half), 1)).astype(BF16)
    place = mxu(earlier, chosen.astype(BF16))
    kept = jnp.where(place == slot.astype(F32), chosen, 0.0)
    return kept, named


def mixer_finish_kernel(
    experts,
    z_ref,
    local_ref,
    carry_ref,
    gain_ref,
    stream_ref,
    weight_ref,
    ffn_gain_ref,
    routes_ref,
    attended_ref,
    dispatched_ref,
    by_member,
    by_group,
    total_ref,
    found,
    entered,
    normed,
    weight,
    partial,
    other,
    weight_sem,
    sent_4,
    got_4,
    *sems,
):
    group, member, core = (lax.axis_index(a) for a in ("grp", "mem", "tp"))
    members, groups = by_member.shape[0], by_group.shape[0]
    barrier = pltpu.get_barrier_semaphore()
    peers = [(group, lax.rem(member + o, members), core) for o in range(1, members)]
    peers += [(lax.rem(group + o, groups), member, core) for o in range(1, groups)]
    peers += [(group, member, 1 - core)]
    for peer in peers:
        pl.semaphore_signal(barrier, inc=1, device_id=peer, device_id_type=MESH)
    depth = weight.shape[0]
    fetch = pltpu.make_async_copy(weight_ref.at[pl.ds(core * depth, depth)], weight, weight_sem)
    fetch.start()
    pl.semaphore_wait(barrier, len(peers))

    copies = entering_states(z_ref, by_member, by_group, total_ref, found, entered, sems)
    normed_heads(local_ref, carry_ref, entered, gain_ref, normed)
    fetch.wait()
    half = stream_ref.shape[0]
    chunks = partial.shape[0]
    mine, theirs = pl.ds(core * half, half), pl.ds((1 - core) * half, half)
    for n in range(chunks):
        partial[n] = jnp.dot(
            normed[...], weight[:, n * COLUMNS : (n + 1) * COLUMNS], preferred_element_type=F32
        )
        copy = remote(
            partial.at[n, theirs],
            other.at[n],
            sent_4.at[n],
            got_4.at[n],
            (group, member, 1 - core),
        )
        copy.start()
        copies.append(copy)
    kept, _ = slot_map(routes_ref, experts, dispatched_ref.shape[0] // experts)
    kept = kept.astype(BF16)
    squares = jnp.zeros((half, 1), F32)
    for n in range(chunks):
        lanes = slice(n * COLUMNS, (n + 1) * COLUMNS)
        copies[n - chunks].wait_recv()
        attended = stream_ref[:, lanes].astype(F32) + (partial[n, mine] + other[n])
        attended_ref[:, lanes] = attended
        squares = squares + jnp.sum(attended * attended, axis=1, keepdims=True)
    width = chunks * COLUMNS
    scaling = lax.rsqrt(squares * (1.0 / width) + NORM_EPS)
    for n in range(chunks):
        lanes = slice(n * COLUMNS, (n + 1) * COLUMNS)
        ffn_in = attended_ref[:, lanes] * scaling * ffn_gain_ref[:, lanes].astype(F32)
        dispatched_ref[:, lanes] = mxu(kept, ffn_in.astype(BF16), ((0,), (0,))).astype(BF16)
    for copy in copies:
        copy.wait_send()


def mixer_finish(z, local_read, carry_read, gain, stream, weight, ffn_gain, routes, experts, capacity):
    half, width = stream.shape
    tokens = local_read.shape[0]
    members, groups = lax.axis_size("mem"), lax.axis_size("grp")
    chunks = width // COLUMNS
    vmem = pl.BlockSpec(memory_space=pltpu.VMEM)
    dma = pltpu.SemaphoreType.DMA
    return pl.pallas_call(
        functools.partial(mixer_finish_kernel, experts),
        in_specs=[vmem] * 5 + [pl.BlockSpec(memory_space=pl.ANY)] + [vmem] * 2,
        out_specs=[vmem, vmem],
        out_shape=[
            jax.ShapeDtypeStruct((half, width), F32),
            jax.ShapeDtypeStruct((experts * capacity, width), BF16),
        ],
        scratch_shapes=[
            pltpu.VMEM((members, 2 * HEAD, LANES), F32),
            pltpu.VMEM((groups, 2 * HEAD, LANES), F32),
            pltpu.VMEM((2 * HEAD, LANES), F32),
            pltpu.VMEM((members, HEAD, LANES), F32),
            pltpu.VMEM((members, HEAD, LANES), F32),
            pltpu.VMEM((tokens, width // 2), BF16),
            pltpu.VMEM((width // 2, width), BF16),
            pltpu.VMEM((chunks, tokens, COLUMNS), F32),
            pltpu.VMEM((chunks, half, COLUMNS), F32),
            dma,
            dma((chunks,)),
            dma((chunks,)),
            dma((members,)),
            dma((members,)),
            dma((groups,)),
            dma((groups,)),
            dma((members,)),
            dma((members,)),
        ],
        compiler_params=pltpu.CompilerParams(
            collective_id=0, has_side_effects=True, vmem_limit_bytes=48 * 1024 * 1024
        ),
        name="mixer_finish",
    )(z, local_read, carry_read, gain, stream, weight, ffn_gain, routes)


PLANES = 4


def plane_offset(step):
    return step + step // 2 * (1 - 2 * (step % 2))


def experts_kernel(
    dispatched_ref,
    attended_ref,
    routes_ref,
    share_ref,
    gate_ref,
    up_ref,
    down_ref,
    out_ref,
    rows,
    gate,
    up,
    down,
    hidden,
    part,
    part_got,
    back_out,
    back,
    fetch_sems,
    own_sems,
    row_sent,
    row_got,
    pass_sent,
    pass_got,
    part_sent,
    part_got_sem,
    back_sent,
    back_got,
):
    group, member, core = (lax.axis_index(a) for a in ("grp", "mem", "tp"))
    members = lax.axis_size("mem")
    chips, experts = back.shape[1], dispatched_ref.shape[0]
    capacity, width = rows.shape[3:]
    floor = chips // PLANES
    side = math.isqrt(floor)
    half_width = width // 2
    chip = group * members + member
    plane, spot = chip // floor, chip % floor

    def at(target, which):
        return (target // members, lax.rem(target, members), which)

    def spot_of(offset):
        return lax.rem(spot // side + offset // side, side) * side + lax.rem(
            lax.rem(spot, side) + lax.rem(offset, side), side
        )

    barrier = pltpu.get_barrier_semaphore()
    devices = 2 * chips

    def greet(offset, carry):
        peer = lax.rem(2 * chip + core + offset, devices)
        pl.semaphore_signal(
            barrier, inc=1, device_id=at(peer // 2, lax.rem(peer, 2)), device_id_type=MESH
        )
        return carry

    lax.fori_loop(1, devices, greet, 0)
    fetches = []
    for n, (source, target) in enumerate(((gate_ref, gate), (up_ref, up), (down_ref, down))):
        fetches.append(pltpu.make_async_copy(source.at[0], target, fetch_sems.at[n]))
        fetches[-1].start()
    own_rows = pltpu.make_async_copy(
        dispatched_ref.at[chip // 2], rows.at[core, plane, spot], own_sems.at[0]
    )
    own_rows.start()
    pl.semaphore_wait(barrier, devices - 1)

    for step in range(PLANES):
        target_plane = lax.rem(plane + plane_offset(step), PLANES)

        def send_rows(offset, carry):
            target = target_plane * floor + spot_of(offset)
            remote(
                dispatched_ref.at[target // 2],
                rows.at[core, plane, spot],
                row_sent.at[step],
                row_got.at[step],
                at(target, core),
            ).start()
            return carry

        lax.fori_loop(1 if step == 0 else 0, floor, send_rows, 0)

    own_rows.wait()
    for copy in fetches:
        copy.wait()

    def row_copies(step, source_plane, count):
        span = rows.at[core, source_plane, pl.ds(0, count)]
        return remote(span, span, row_sent.at[step], row_got.at[step], at(chip, 1 - core))

    def passing(step, source_plane, side_core):
        span = rows.at[side_core, source_plane]
        return remote(span, span, pass_sent.at[step], pass_got.at[step], at(chip, 1 - core))

    def part_copy(step):
        return remote(
            part.at[step, 1 - core],
            part_got.at[step],
            part_sent.at[step],
            part_got_sem.at[step],
            at(chip, 1 - core),
        )

    def back_copy(step, source_plane, which, offset):
        target = source_plane * floor + spot_of(offset)
        return remote(
            back_out.at[step, which, lax.rem(target, floor)],
            back.at[core, chip],
            back_sent.at[step],
            back_got.at[core],
            at(target, which),
        )

    def plane_of(step):
        return lax.rem(plane + PLANES - plane_offset(step), PLANES)

    def compute(step, source_plane):
        held = rows[:, source_plane].reshape(2 * floor * capacity, width)
        inner = gate.shape[1]
        for start in range(0, inner, 256):
            lanes = slice(start, min(start + 256, inner))
            gate_act = mxu(held, gate[:, lanes])
            up_act = mxu(held, up[:, lanes])
            hidden[:, lanes] = (gate_act * jax.nn.sigmoid(gate_act) * up_act).astype(BF16)
        for side_at in range(2):
            for start in range(0, half_width, 512):
                lanes = slice(start, min(start + 512, half_width))
                columns = slice(side_at * half_width + lanes.start, side_at * half_width + lanes.stop)
                part[step, side_at, :, lanes] = mxu(hidden[...], down[:, columns]).astype(BF16)

    def finish(step):
        source_plane = plane_of(step)
        part_copy(step).wait_recv()
        total = part[step, core].astype(F32) + part_got[step].astype(F32)
        back_out[step] = total.astype(BF16).reshape(2, floor, capacity, half_width)

        def send_back(offset, carry):
            back_copy(step, source_plane, 1 - core, offset).start()
            return carry

        def send_same(offset, carry):
            back_copy(step, source_plane, core, offset).start()
            return carry

        lax.fori_loop(0, floor, send_back, 0)
        if isinstance(step, int) and step == 0:
            lax.fori_loop(1, floor, send_same, 0)
            own = pltpu.make_async_copy(
                back_out.at[0, core, spot], back.at[core, chip], own_sems.at[1]
            )
            own.start()
            own.wait()
        else:
            lax.fori_loop(0, floor, send_same, 0)

    for step in range(PLANES):
        source_plane = plane_of(step)
        row_copies(step, source_plane, floor - 1 if step == 0 else floor).wait_recv()
        passing(step, source_plane, core).start()
        passing(step, source_plane, 1 - core).wait_recv()
        compute(step, source_plane)
        part_copy(step).start()
        if step > 0:
            finish(step - 1)
    finish(PLANES - 1)

    kept, named = slot_map(routes_ref, experts, capacity)
    shares = kept * jnp.where(named[0], share_ref[:, 0:1], share_ref[:, 1:2])
    shares = packed(split(shares))
    for turn in range(2):
        which = 1 - core if turn == 0 else core
        span = back.at[which, pl.ds(0, chips - turn)]
        remote(span, span, back_sent.at[0], back_got.at[which], at(chip, 1 - core)).wait_recv()
    for which in range(2):
        lanes = slice(which * half_width, (which + 1) * half_width)
        pair = back[which].reshape(experts, 2, capacity, half_width).astype(F32)
        whole = (pair[:, 0] + pair[:, 1]).astype(BF16).reshape(experts * capacity, half_width)
        mixture = mxu(shares, jnp.concatenate((whole, whole), axis=0))
        out_ref[:, lanes] = (attended_ref[:, lanes] + mixture).astype(BF16)

    for step in range(PLANES):
        source_plane = plane_of(step)
        row_copies(step, source_plane, floor - 1 if step == 0 else floor).wait_send()
        passing(step, source_plane, core).wait_send()
        part_copy(step).wait_send()
        if step == 0:
            sent = back_out.at[step, 0]
            remote(sent, sent, back_sent.at[step], back_got.at[0], at(chip, 1 - core)).wait_send()
            if floor > 1:
                sent = back_out.at[step, 0, pl.ds(0, floor - 1)]
                remote(sent, sent, back_sent.at[step], back_got.at[0], at(chip, 1 - core)).wait_send()
        else:
            sent = back_out.at[step]
            remote(sent, sent, back_sent.at[step], back_got.at[0], at(chip, 1 - core)).wait_send()


def routed_experts(dispatched, attended, routes, shares, gate, up, down):
    experts, capacity, width = dispatched.shape
    half = attended.shape[0]
    chips = 2 * experts
    inner = gate.shape[2]
    floor = chips // PLANES
    rows_step = 2 * floor * capacity
    vmem = pl.BlockSpec(memory_space=pltpu.VMEM)
    hbm = pl.BlockSpec(memory_space=pl.ANY)
    dma = pltpu.SemaphoreType.DMA
    return pl.pallas_call(
        experts_kernel,
        in_specs=[vmem] * 4 + [hbm] * 3,
        out_specs=vmem,
        out_shape=jax.ShapeDtypeStruct((half, width), BF16),
        scratch_shapes=[
            pltpu.VMEM((2, PLANES, floor, capacity, width), BF16),
            pltpu.VMEM((width, inner), BF16),
            pltpu.VMEM((width, inner), BF16),
            pltpu.VMEM((inner, width), BF16),
            pltpu.VMEM((rows_step, inner), BF16),
            pltpu.VMEM((PLANES, 2, rows_step, width // 2), BF16),
            pltpu.VMEM((PLANES, rows_step, width // 2), BF16),
            pltpu.VMEM((PLANES, 2, floor, capacity, width // 2), BF16),
            pltpu.VMEM((2, chips, capacity, width // 2), BF16),
            dma((3,)),
            dma((2,)),
        ]
        + [dma((PLANES,))] * 7
        + [dma((2,))],
        compiler_params=pltpu.CompilerParams(
            collective_id=1, has_side_effects=True, vmem_limit_bytes=58 * 1024 * 1024
        ),
        name="routed_experts",
    )(dispatched, attended, routes, shares, gate, up, down)


TOPK = 2
SP_TP = ("grp", "mem", "tp")
SP = ("grp", "mem")


def local(
    stream_in,
    query_rows,
    key_rows,
    value_rows,
    removal_key,
    learn_pre,
    log_rate,
    norm_gain,
    out_weight,
    ffn_gain,
    routes,
    route_weight,
    expert_gate,
    expert_up,
    expert_down,
):
    half_rows, width = stream_in.shape
    experts = lax.axis_size(SP) // 2
    capacity = 2 * TOPK * half_rows // experts
    z, local_read, carry_read = mixer_blocks(
        query_rows, key_rows, value_rows, removal_key, learn_pre, log_rate, per_step=4
    )
    attended, dispatched = mixer_finish(
        z,
        local_read,
        carry_read,
        norm_gain.reshape(1, -1),
        stream_in,
        out_weight,
        ffn_gain.reshape(1, -1),
        routes,
        experts,
        capacity,
    )
    return routed_experts(
        dispatched.reshape(experts, capacity, width),
        attended,
        routes,
        route_weight,
        expert_gate,
        expert_up,
        expert_down,
    )


def solution(mesh):
    sp = mesh.shape["sp"]
    groups = 1
    while groups * groups < sp:
        groups *= 2
    torus = Mesh(
        mesh.devices.reshape(sp // groups, groups, mesh.shape["tp"]), ("grp", "mem", "tp")
    )
    return jax.shard_map(
        local,
        mesh=torus,
        in_specs=(
            P(SP_TP, None),
            P(SP, "tp"),
            P(SP, "tp"),
            P(SP, "tp"),
            P(SP, "tp"),
            P(SP, "tp"),
            P(SP, "tp"),
            P("tp"),
            P(),
            P(),
            P(SP_TP, None),
            P(SP_TP, None),
            P(SP, None, "tp"),
            P(SP, None, "tp"),
            P(SP, "tp", None),
        ),
        out_specs=P(SP_TP, None),
        check_vma=False,
    )
```

```python
from typing import NamedTuple

import jax
import jax.numpy as jnp
from jax import lax
from jax.experimental import pallas as pl
from jax.experimental.pallas import tpu as pltpu
from jax.sharding import Mesh
from jax.sharding import PartitionSpec as P

HEAD = 64
LANES = 128
F32 = jnp.float32
BF16 = jnp.bfloat16
UNIT_EPS = 1e-06


def split(x):
    high = x.astype(BF16)
    return high, (x - high.astype(F32)).astype(BF16)


def mxu(x, y, dims=((1,), (0,))):
    return lax.dot_general(x, y, (dims, ((), ())), preferred_element_type=F32)


def packed(x):
    return jnp.concatenate(x, axis=1)


def spread(y):
    high, low = y
    top = jnp.concatenate((high, low), axis=1)
    return jnp.concatenate((top, top), axis=0)


def folded(z):
    half = z.shape[1] // 2
    return z[:, :half] + z[:, half:]


def product(x, y):
    return folded(mxu(packed(x), spread(y)))


def iota(shape, dim):
    return lax.broadcasted_iota(jnp.int32, shape, dim)


class Masks(NamedTuple):
    same_head: jax.Array
    lower: jax.Array


class Prepared(NamedTuple):
    left: list
    right: list
    values: jax.Array
    starts: jax.Array
    query_now: jax.Array
    pull_tail: jax.Array
    key_tail: jax.Array
    decay_all: jax.Array


def mixer_prepare(refs, lanes, masks):
    q_ref, k_ref, v_ref, r_ref, l_ref, g_ref = refs
    tokens = q_ref.shape[0]
    removal = r_ref[:, lanes].astype(F32)
    squares = split(removal * removal)
    total = mxu(packed(squares), jnp.concatenate((masks.same_head, masks.same_head), axis=0))
    unit = removal * lax.rsqrt(total + UNIT_EPS)
    pull = unit * jax.nn.sigmoid(l_ref[:, lanes].astype(F32))
    log_decay = -jnp.exp(g_ref[:, lanes])
    high = log_decay.astype(BF16)
    rest = log_decay - high.astype(F32)
    mid = rest.astype(BF16)
    low = (rest - mid.astype(F32)).astype(BF16)
    stacked = jnp.concatenate((packed((high, mid)), packed((low, jnp.zeros_like(low)))), axis=0)
    cumul = folded(mxu(packed((masks.lower, masks.lower)), stacked))
    middle = cumul[tokens // 2 - 1 : tokens // 2]
    end = cumul[tokens - 1 : tokens]
    grown = jnp.exp(middle - cumul)
    faded = jnp.exp(cumul - middle)
    unit_hat = unit * jnp.exp(cumul - log_decay - middle)
    query_hat = q_ref[:, lanes].astype(F32) * faded
    pull_hat = pull * grown
    key_hat = k_ref[:, lanes].astype(F32) * grown
    from_start = jnp.exp(middle)
    to_end = jnp.exp(end - middle)
    values = v_ref[:, lanes]
    left = [jnp.concatenate(p, axis=0) for p in zip(split(unit_hat), split(query_hat))]
    right = [jnp.concatenate(p, axis=0) for p in zip(split(pull_hat), split(key_hat))]
    return Prepared(
        left,
        right,
        jnp.concatenate((values, values), axis=0),
        pltpu.roll(unit_hat * from_start, HEAD, 1),
        query_hat * from_start,
        spread(split(pull_hat * to_end)),
        jnp.concatenate(split(key_hat * to_end), axis=0),
        jnp.exp(end),
    )


def mixer_kernel(pairs, q_ref, k_ref, v_ref, r_ref, l_ref, g_ref, z_ref, local_ref, carry_ref):
    refs = (q_ref, k_ref, v_ref, r_ref, l_ref, g_ref)
    tokens = q_ref.shape[0]
    row, col = iota((tokens, tokens), 0), iota((tokens, tokens), 1)
    strict, upto, apart = row > col, row >= col, row ^ col
    first = iota((tokens, LANES), 1) < HEAD
    masks = Masks(
        ((iota((LANES, LANES), 0) < HEAD) == (iota((LANES, LANES), 1) < HEAD)).astype(BF16),
        upto.astype(BF16),
    )
    own_lanes = (first, jnp.logical_not(first))
    lanes = [slice(pair * LANES, (pair + 1) * LANES) for pair in range(pairs)]
    ready = [mixer_prepare(refs, part, masks) for part in lanes]
    heads = [(pair, head) for pair in range(pairs) for head in range(2)]

    scores = []
    for pair, head in heads:
        inside = jnp.concatenate((own_lanes[head], own_lanes[head]), axis=0)
        own = [jnp.where(inside, x, jnp.zeros_like(x)) for x in ready[pair].left]
        right = ready[pair].right
        scores.append(
            mxu(packed(own), packed((right[0], right[0])), ((1,), (1,)))
            + mxu(own[0], right[1], ((1,), (1,)))
        )
    mix_pull = [jnp.where(strict, s[:tokens, :tokens], 0.0) for s in scores]
    mix_key = [jnp.where(strict, s[:tokens, tokens:], 0.0) for s in scores]
    read_pull = [split(jnp.where(upto, s[tokens:, :tokens], 0.0)) for s in scores]
    read_key = [jnp.where(upto, s[tokens:, tokens:], 0.0) for s in scores]
    by_key = []
    for n, (pair, head) in enumerate(heads):
        both = [jnp.concatenate(p, axis=0) for p in zip(split(mix_key[n]), split(read_key[n]))]
        by_key.append(mxu(packed(both), ready[pair].values))

    identity = (row == col).astype(F32)
    inverse = [identity - jnp.where(apart < 2, m, 0.0) for m in mix_pull]
    size = 2
    while size < tokens:
        within = (apart >= size) & (apart < 2 * size)
        parts = [split(x) for x in inverse]
        edges = [split(jnp.where(within, m, 0.0)) for m in mix_pull]
        steps = [split(product(x, y)) for x, y in zip(parts, edges)]
        inverse = [x - product(y, z) for x, y, z in zip(inverse, steps, parts)]
        size *= 2

    answers, solved, outer = [], [], []
    for n, (pair, head) in enumerate(heads):
        sources = jnp.where(own_lanes[head], by_key[n][:tokens], ready[pair].starts)
        answers.append(split(product(split(inverse[n]), split(sources))))
    for n, (pair, head) in enumerate(heads):
        solved.append(product(read_pull[n], answers[n]))
        stacked = jnp.concatenate(answers[n], axis=0)
        outer.append(folded(mxu(stacked, ready[pair].pull_tail, ((0,), (0,)))))

    half = iota((HEAD, LANES), 1) < HEAD
    diagonal = (iota((HEAD, LANES), 1) % HEAD) == iota((HEAD, LANES), 0)
    for pair in range(pairs):
        one, two = 2 * pair, 2 * pair + 1
        local_ref[:, lanes[pair]] = jnp.where(
            first, by_key[one][tokens:] - solved[one], by_key[two][tokens:] - solved[two]
        )
        carry_ref[:, lanes[pair]] = ready[pair].query_now - pltpu.roll(
            jnp.where(first, solved[two], solved[one]), HEAD, 1
        )
        written = mxu(ready[pair].values, ready[pair].key_tail, ((0,), (0,)))
        z_ref[pair, :HEAD] = jnp.where(
            half, written[:HEAD] - outer[one][:HEAD], written[HEAD:] - outer[two][HEAD:]
        )
        z_ref[pair, HEAD:] = jnp.where(diagonal, ready[pair].decay_all, 0.0) - jnp.where(
            half, outer[one][HEAD:], outer[two][:HEAD]
        )


MESH = pl.DeviceIdType.MESH
GROUP_EPS = 0.00064
NORM_EPS = 1e-06
COLUMNS = 512


def block_diagonal(rows):
    first = iota(rows.shape, 1) < HEAD
    zero = jnp.zeros_like(rows)
    return jnp.concatenate((jnp.where(first, rows, zero), jnp.where(first, zero, rows)), axis=0)


def mapped(earlier, later):
    return product(split(earlier), split(block_diagonal(later[HEAD:])))


def compose(earlier, later):
    joined = mapped(earlier, later)
    return jnp.concatenate((joined[:HEAD] + later[:HEAD], joined[HEAD:]), axis=0)


def prefixes(blocks):
    done, step = list(blocks), 1
    while step < len(done):
        for j in range(len(done)):
            if (j // step) % 2 == 1:
                done[j] = compose(done[j // step * step - 1], done[j])
        step *= 2
    return done


def joined_all(blocks):
    while len(blocks) > 1:
        pairs = [compose(*blocks[j : j + 2]) for j in range(0, len(blocks) - 1, 2)]
        blocks = pairs + (blocks[-1:] if len(blocks) % 2 else [])
    return blocks[0]


def remote(source, target, sends, receives, place):
    return pltpu.make_async_remote_copy(
        src_ref=source,
        dst_ref=target,
        send_sem=sends,
        recv_sem=receives,
        device_id=place,
        device_id_type=MESH,
    )


def entering_states(z_ref, by_member, by_group, total_ref, found, entered, sems):
    group, member, core = (lax.axis_index(a) for a in ("grp", "mem", "tp"))
    members, groups = by_member.shape[0], by_group.shape[0]
    sent_1, got_1, sent_2, got_2, sent_3, got_3 = sems

    first = []
    for offset in range(1, members):
        peer = lax.rem(member + offset, members)
        copy = remote(
            z_ref.at[peer],
            by_member.at[member],
            sent_1.at[offset],
            got_1.at[member],
            (group, peer, core),
        )
        copy.start()
        first.append(copy)
    by_member[member] = z_ref[member]
    for offset in range(1, members):
        peer = lax.rem(member + offset, members)
        remote(
            z_ref.at[peer], by_member.at[peer], sent_1.at[offset], got_1.at[peer], (group, peer, core)
        ).wait_recv()
    inclusive = prefixes([by_member[j] for j in range(members)])
    total_ref[...] = inclusive[-1]

    second = []
    for offset in range(1, groups):
        peer = lax.rem(group + offset, groups)
        copy = remote(
            total_ref,
            by_group.at[group],
            sent_2.at[offset],
            got_2.at[group],
            (peer, member, core),
        )
        copy.start()
        second.append(copy)
    maps = [spread(split(block_diagonal(inclusive[j][HEAD:]))) for j in range(members - 1)]
    by_group[group] = total_ref[...]
    for offset in range(1, groups):
        peer = lax.rem(group + offset, groups)
        remote(
            total_ref, by_group.at[peer], sent_2.at[offset], got_2.at[peer], (peer, member, core)
        ).wait_recv()
    shape = total_ref.shape
    neutral = ((iota(shape, 1) % HEAD) + HEAD == iota(shape, 0)).astype(F32)
    before = [jnp.where(j < group, by_group[j], neutral) for j in range(groups - 1)]
    start = joined_all(before)[:HEAD]
    parts = packed(split(start))
    found[0] = start
    for j in range(1, members):
        found[j] = folded(mxu(parts, maps[j - 1])) + inclusive[j - 1][:HEAD]

    third = []
    for offset in range(1, members):
        peer = lax.rem(member + offset, members)
        copy = remote(
            found.at[peer],
            entered.at[member],
            sent_3.at[offset],
            got_3.at[member],
            (group, peer, core),
        )
        copy.start()
        third.append(copy)
    entered[member] = found[member]
    for offset in range(1, members):
        peer = lax.rem(member + offset, members)
        remote(
            found.at[peer], entered.at[peer], sent_3.at[offset], got_3.at[peer], (group, peer, core)
        ).wait_recv()
    return first + second + third


def normed_heads(local_ref, carry_ref, entered, gain_ref, normed):
    same_head = ((iota((LANES, LANES), 0) < HEAD) == (iota((LANES, LANES), 1) < HEAD)).astype(BF16)
    same_head = jnp.concatenate((same_head, same_head), axis=0)
    pairs = entered.shape[0]
    per_step = pairs // local_ref.shape[0]
    lanes = [slice(pair * LANES, (pair + 1) * LANES) for pair in range(pairs)]
    mixed = []
    for pair in range(pairs):
        high, low = split(block_diagonal(entered[pair]))
        rhs = jnp.concatenate((packed((high, high)), packed((low, low))), axis=0)
        step, held = pair // per_step, lanes[pair % per_step]
        read = folded(mxu(packed(split(carry_ref[step, :, held])), rhs, ((1,), (1,))))
        mixed.append(local_ref[step, :, held] + read)
    centred = [x - mxu(packed(split(x)), same_head) * (1.0 / HEAD) for x in mixed]
    variance = [mxu(packed(split(x * x)), same_head) * (1.0 / HEAD) for x in centred]
    for pair in range(pairs):
        scaled = centred[pair] * lax.rsqrt(variance[pair] + GROUP_EPS)
        normed[:, lanes[pair]] = (scaled * gain_ref[:, lanes[pair]].astype(F32)).astype(BF16)


def slot_map(routes_ref, experts, capacity):
    half = routes_ref.shape[1]
    shape = (experts * capacity, half)
    place = iota(shape, 0)
    expert, slot = place // capacity, place % capacity
    named = [routes_ref[k : k + 1, :] == expert for k in range(2)]
    chosen = (named[0] | named[1]).astype(F32)
    earlier = (iota((half, half), 0) < iota((half, half), 1)).astype(BF16)
    count = mxu(chosen.astype(BF16), earlier)
    return jnp.where(count == slot.astype(F32), chosen, 0.0), named


SP_TP = ("grp", "mem", "tp")
SP = ("grp", "mem")
STEPS = 2
GROUPS = 4


def far_first(side):
    offsets = [(z, y, x) for z in range(side) for y in range(side) for x in range(side)]
    return sorted(offsets, key=lambda o: -sum(min(d, side - d) for d in o))


def layer_kernel(
    q_ref,
    k_ref,
    v_ref,
    r_ref,
    l_ref,
    g_ref,
    stream_ref,
    weight_ref,
    gate_ref,
    up_ref,
    down_ref,
    gain_ref,
    ffn_gain_ref,
    routes_ref,
    share_ref,
    out_ref,
    q,
    k,
    v,
    r,
    l,
    g,
    stream,
    weight,
    gate,
    up,
    down,
    z,
    local_read,
    carry_read,
    by_member,
    by_group,
    total_ref,
    found,
    entered,
    normed,
    partial,
    other,
    attended,
    dispatched,
    rows,
    hidden,
    part,
    part_got,
    back_out,
    back,
    in_sems,
    fetch_sems,
    sent_1,
    got_1,
    sent_2,
    got_2,
    sent_3,
    got_3,
    sent_4,
    got_4,
    row_sent,
    row_got,
    pass_sent,
    pass_got,
    part_sent,
    part_arrived,
    back_sent,
    back_got,
):
    group, member, core = (lax.axis_index(a) for a in ("grp", "mem", "tp"))
    members = lax.axis_size("mem")
    chips, experts = back.shape[1], dispatched.shape[0]
    capacity, width = rows.shape[2:]
    half_width = width // 2
    chip = group * members + member
    sibling = (group, member, 1 - core)

    def at(target, which):
        return (target // members, lax.rem(target, members), which)

    barrier = pltpu.get_barrier_semaphore()
    devices = 2 * chips

    def greet(offset, carry):
        peer = lax.rem(2 * chip + core + offset, devices)
        pl.semaphore_signal(
            barrier, inc=1, device_id=at(peer // 2, lax.rem(peer, 2)), device_id_type=MESH
        )
        return carry

    held = q.shape[2]
    loads = []
    for step in range(STEPS):
        lanes = pl.ds(step * held, held)
        for n, (source, target) in enumerate(
            ((q_ref, q), (k_ref, k), (v_ref, v), (r_ref, r), (l_ref, l), (g_ref, g))
        ):
            loads.append(
                pltpu.make_async_copy(source.at[:, lanes], target.at[step], in_sems.at[step, n])
            )
            loads[-1].start()
    depth = weight.shape[0]
    fetches = []
    for n, (source, target) in enumerate(
        (
            (stream_ref, stream),
            (weight_ref.at[pl.ds(core * depth, depth)], weight),
            (gate_ref.at[0], gate),
            (up_ref.at[0], up),
            (down_ref.at[0], down),
        )
    ):
        fetches.append(pltpu.make_async_copy(source, target, fetch_sems.at[n]))
    lax.fori_loop(1, devices, greet, 0)
    for copy in loads[: len(loads) // STEPS]:
        copy.wait()
    for copy in fetches:
        copy.start()

    pairs = z.shape[0] // STEPS

    def mix(step):
        mixer_kernel(
            pairs,
            *(ref.at[step] for ref in (q, k, v, r, l, g)),
            z.at[pl.ds(step * pairs, pairs)],
            local_read.at[step],
            carry_read.at[step],
        )

    mix(0)
    for copy in loads[len(loads) // STEPS :]:
        copy.wait()
    mix(1)
    pl.semaphore_wait(barrier, devices - 1)

    sems = (sent_1, got_1, sent_2, got_2, sent_3, got_3)
    copies = entering_states(z, by_member, by_group, total_ref, found, entered, sems)
    normed_heads(local_read, carry_read, entered, gain_ref, normed)
    fetches[0].wait()
    fetches[1].wait()
    half = stream.shape[0]
    chunks = partial.shape[0]
    mine, theirs = pl.ds(core * half, half), pl.ds((1 - core) * half, half)
    shared = []
    for n in range(chunks):
        partial[n] = jnp.dot(
            normed[...], weight[:, n * COLUMNS : (n + 1) * COLUMNS], preferred_element_type=F32
        )
        shared.append(
            remote(partial.at[n, theirs], other.at[n], sent_4.at[n], got_4.at[n], sibling)
        )
        shared[-1].start()
    kept, named = slot_map(routes_ref, experts, capacity)
    picks = kept.astype(BF16)
    shares = kept * jnp.where(named[0], share_ref[0:1, :], share_ref[1:2, :])
    shares = jnp.concatenate(split(shares), axis=0)
    squares = jnp.zeros((half, 1), F32)
    for n in range(chunks):
        lanes = slice(n * COLUMNS, (n + 1) * COLUMNS)
        shared[n].wait_recv()
        block = stream[:, lanes].astype(F32) + (partial[n, mine] + other[n])
        attended[:, lanes] = block
        squares = squares + jnp.sum(block * block, axis=1, keepdims=True)
    scaling = lax.rsqrt(squares * (1.0 / width) + NORM_EPS)
    for n in range(chunks):
        lanes = slice(n * COLUMNS, (n + 1) * COLUMNS)
        ffn_in = attended[:, lanes] * scaling * ffn_gain_ref[:, lanes].astype(F32)
        sent_rows = mxu(picks, ffn_in.astype(BF16)).astype(BF16)
        dispatched[:, :, lanes] = sent_rows.reshape(experts, capacity, COLUMNS)

    side = round(chips ** (1 / 3))
    order = far_first(side)
    here = (chip // (side * side), chip // side % side, chip % side)

    def shifted(offset, sign):
        place = [lax.rem(h + side + sign * o, side) for h, o in zip(here, offset)]
        return (place[0] * side + place[1]) * side + place[2]

    span = chips // GROUPS
    rows[core, chips - 1] = dispatched[chip // 2]
    for n, offset in enumerate(order[:-1]):
        target = shifted(offset, 1)
        remote(
            dispatched.at[target // 2],
            rows.at[core, n],
            row_sent.at[n // span],
            row_got.at[n // span],
            at(target, core),
        ).start()
    for copy in fetches[2:]:
        copy.wait()

    def row_copies(step):
        count = span - 1 if step == GROUPS - 1 else span
        held = rows.at[core, pl.ds(step * span, count)]
        return remote(held, held, row_sent.at[step], row_got.at[step], sibling)

    def passing(step, which):
        held = rows.at[which, pl.ds(step * span, span)]
        return remote(held, held, pass_sent.at[step], pass_got.at[step], sibling)

    def part_copy(step):
        return remote(
            part.at[step, 1 - core],
            part_got.at[step],
            part_sent.at[step],
            part_arrived.at[step],
            sibling,
        )

    def compute(step):
        taken = rows[:, step * span : (step + 1) * span].reshape(2 * span * capacity, width)
        inner = gate.shape[1]
        for start in range(0, inner, 256):
            lanes = slice(start, min(start + 256, inner))
            gate_act = mxu(taken, gate[:, lanes])
            up_act = mxu(taken, up[:, lanes])
            hidden[:, lanes] = (gate_act * jax.nn.sigmoid(gate_act) * up_act).astype(BF16)
        for which in range(2):
            for start in range(0, half_width, COLUMNS):
                columns = slice(which * half_width + start, which * half_width + start + COLUMNS)
                part[step, which, :, start : start + COLUMNS] = mxu(
                    hidden[...], down[:, columns]
                ).astype(BF16)

    def finish(step):
        part_copy(step).wait_recv()
        total = part[step, core].astype(F32) + part_got[step].astype(F32)
        back_out[step] = total.astype(BF16).reshape(2, span, capacity, half_width)
        for n in range(span):
            offset = order[step * span + n]
            target = shifted(offset, -1)
            for turn in range(2):
                which = 1 - core if turn == 0 else core
                if turn == 1 and not any(offset):
                    back[core, chip] = back_out[step, core, n]
                    continue
                remote(
                    back_out.at[step, which, n],
                    back.at[core, chip],
                    back_sent.at[step],
                    back_got.at[core],
                    at(target, which),
                ).start()

    for step in range(GROUPS):
        row_copies(step).wait_recv()
        passing(step, core).start()
        passing(step, 1 - core).wait_recv()
        compute(step)
        part_copy(step).start()
        if step > 0:
            finish(step - 1)
    finish(GROUPS - 1)

    def all_back(ref, sem_sent, sem_got):
        return remote(ref, ref, sem_sent, sem_got, sibling)

    for turn in range(2):
        which = 1 - core if turn == 0 else core
        all_back(back.at[which, pl.ds(0, chips - turn)], back_sent.at[0], back_got.at[which]).wait_recv()
    for which in range(2):
        lanes = slice(which * half_width, (which + 1) * half_width)
        both = back[which].reshape(experts, 2, capacity, half_width).astype(F32)
        whole = (both[:, 0] + both[:, 1]).astype(BF16).reshape(experts * capacity, half_width)
        mixture = mxu(shares, jnp.concatenate((whole, whole), axis=0), ((0,), (0,)))
        out_ref[:, lanes] = (attended[:, lanes] + mixture).astype(BF16)

    for copy in copies + shared:
        copy.wait_send()
    for step in range(GROUPS):
        row_copies(step).wait_send()
        passing(step, core).wait_send()
        part_copy(step).wait_send()
        last = 1 if step == GROUPS - 1 else 0
        all_back(back_out.at[step, 0], back_sent.at[step], back_got.at[0]).wait_send()
        all_back(
            back_out.at[step, 1, pl.ds(0, span - last)], back_sent.at[step], back_got.at[0]
        ).wait_send()


def local(
    stream_in,
    query_rows,
    key_rows,
    value_rows,
    removal_key,
    learn_pre,
    log_rate,
    norm_gain,
    out_weight,
    ffn_gain,
    routes,
    route_weight,
    expert_gate,
    expert_up,
    expert_down,
):
    half, width = stream_in.shape
    tokens, own_width = query_rows.shape
    chips = lax.axis_size(("grp", "mem"))
    members, groups = lax.axis_size("mem"), lax.axis_size("grp")
    experts = chips // 2
    capacity = 2 * routes.shape[1] * half // experts
    inner = expert_gate.shape[2]
    span = chips // GROUPS
    held = own_width // STEPS
    pairs = own_width // LANES
    chunks = width // COLUMNS
    taken = 2 * span * capacity
    vmem = pl.BlockSpec(memory_space=pltpu.VMEM)
    hbm = pl.BlockSpec(memory_space=pl.ANY)
    dma = pltpu.SemaphoreType.DMA
    return pl.pallas_call(
        layer_kernel,
        in_specs=[hbm] * 11 + [vmem] * 4,
        out_specs=vmem,
        out_shape=jax.ShapeDtypeStruct((half, width), BF16),
        scratch_shapes=[pltpu.VMEM((STEPS, tokens, held), BF16)] * 5
        + [
            pltpu.VMEM((STEPS, tokens, held), F32),
            pltpu.VMEM((half, width), BF16),
            pltpu.VMEM((width // 2, width), BF16),
            pltpu.VMEM((width, inner), BF16),
            pltpu.VMEM((width, inner), BF16),
            pltpu.VMEM((inner, width), BF16),
            pltpu.VMEM((pairs, 2 * HEAD, LANES), F32),
            pltpu.VMEM((STEPS, tokens, held), F32),
            pltpu.VMEM((STEPS, tokens, held), F32),
            pltpu.VMEM((members, 2 * HEAD, LANES), F32),
            pltpu.VMEM((groups, 2 * HEAD, LANES), F32),
            pltpu.VMEM((2 * HEAD, LANES), F32),
            pltpu.VMEM((members, HEAD, LANES), F32),
            pltpu.VMEM((members, HEAD, LANES), F32),
            pltpu.VMEM((tokens, own_width), BF16),
            pltpu.VMEM((chunks, tokens, COLUMNS), F32),
            pltpu.VMEM((chunks, half, COLUMNS), F32),
            pltpu.VMEM((half, width), F32),
            pltpu.VMEM((experts, capacity, width), BF16),
            pltpu.VMEM((2, chips, capacity, width), BF16),
            pltpu.VMEM((taken, inner), BF16),
            pltpu.VMEM((GROUPS, 2, taken, width // 2), BF16),
            pltpu.VMEM((GROUPS, taken, width // 2), BF16),
            pltpu.VMEM((GROUPS, 2, span, capacity, width // 2), BF16),
            pltpu.VMEM((2, chips, capacity, width // 2), BF16),
            dma((STEPS, 6)),
            dma((5,)),
            dma((members,)),
            dma((members,)),
            dma((groups,)),
            dma((groups,)),
            dma((members,)),
            dma((members,)),
            dma((chunks,)),
            dma((chunks,)),
        ]
        + [dma((GROUPS,))] * 7
        + [dma((2,))],
        compiler_params=pltpu.CompilerParams(
            collective_id=0, has_side_effects=True, vmem_limit_bytes=63 * 1024 * 1024
        ),
        name="layer",
    )(
        query_rows,
        key_rows,
        value_rows,
        removal_key,
        learn_pre,
        log_rate,
        stream_in,
        out_weight,
        expert_gate,
        expert_up,
        expert_down,
        norm_gain.reshape(1, -1),
        ffn_gain.reshape(1, -1),
        routes.T,
        route_weight.T,
    )


def solution(mesh):
    sp = mesh.shape["sp"]
    groups = 1
    while groups * groups < sp:
        groups *= 2
    torus = Mesh(
        mesh.devices.reshape(sp // groups, groups, mesh.shape["tp"]), ("grp", "mem", "tp")
    )
    return jax.shard_map(
        local,
        mesh=torus,
        in_specs=(
            P(SP_TP, None),
            P(SP, "tp"),
            P(SP, "tp"),
            P(SP, "tp"),
            P(SP, "tp"),
            P(SP, "tp"),
            P(SP, "tp"),
            P("tp"),
            P(),
            P(),
            P(SP_TP, None),
            P(SP_TP, None),
            P(SP, None, "tp"),
            P(SP, None, "tp"),
            P(SP, "tp", None),
        ),
        out_specs=P(SP_TP, None),
        check_vma=False,
    )
```

```python
from typing import NamedTuple

import jax
import jax.numpy as jnp
from jax import lax
from jax.experimental import pallas as pl
from jax.experimental.pallas import tpu as pltpu
from jax.sharding import Mesh
from jax.sharding import PartitionSpec as P

HEAD = 64
LANES = 128
F32 = jnp.float32
BF16 = jnp.bfloat16
UNIT_EPS = 1e-06


def split(x):
    high = x.astype(BF16)
    return high, (x - high.astype(F32)).astype(BF16)


def mxu(x, y, dims=((1,), (0,))):
    return lax.dot_general(x, y, (dims, ((), ())), preferred_element_type=F32)


def packed(x):
    return jnp.concatenate(x, axis=1)


def spread(y):
    high, low = y
    top = jnp.concatenate((high, low), axis=1)
    return jnp.concatenate((top, top), axis=0)


def folded(z):
    half = z.shape[1] // 2
    return z[:, :half] + z[:, half:]


def product(x, y):
    return folded(mxu(packed(x), spread(y)))


def iota(shape, dim):
    return lax.broadcasted_iota(jnp.int32, shape, dim)


class Masks(NamedTuple):
    same_head: jax.Array
    lower: jax.Array


class Prepared(NamedTuple):
    left: list
    right: list
    values: jax.Array
    starts: jax.Array
    query_now: jax.Array
    pull_tail: jax.Array
    key_tail: jax.Array
    decay_all: jax.Array


def mixer_prepare(refs, lanes, masks):
    q_ref, k_ref, v_ref, r_ref, l_ref, g_ref = refs
    tokens = q_ref.shape[0]
    removal = r_ref[:, lanes].astype(F32)
    squares = split(removal * removal)
    total = mxu(packed(squares), jnp.concatenate((masks.same_head, masks.same_head), axis=0))
    unit = removal * lax.rsqrt(total + UNIT_EPS)
    pull = unit * jax.nn.sigmoid(l_ref[:, lanes].astype(F32))
    log_decay = -jnp.exp(g_ref[:, lanes])
    high = log_decay.astype(BF16)
    rest = log_decay - high.astype(F32)
    mid = rest.astype(BF16)
    low = (rest - mid.astype(F32)).astype(BF16)
    stacked = jnp.concatenate((packed((high, mid)), packed((low, jnp.zeros_like(low)))), axis=0)
    cumul = folded(mxu(packed((masks.lower, masks.lower)), stacked))
    middle = cumul[tokens // 2 - 1 : tokens // 2]
    end = cumul[tokens - 1 : tokens]
    grown = jnp.exp(middle - cumul)
    faded = jnp.exp(cumul - middle)
    unit_hat = unit * jnp.exp(cumul - log_decay - middle)
    query_hat = q_ref[:, lanes].astype(F32) * faded
    pull_hat = pull * grown
    key_hat = k_ref[:, lanes].astype(F32) * grown
    from_start = jnp.exp(middle)
    to_end = jnp.exp(end - middle)
    values = v_ref[:, lanes]
    left = [jnp.concatenate(p, axis=0) for p in zip(split(unit_hat), split(query_hat))]
    right = [jnp.concatenate(p, axis=0) for p in zip(split(pull_hat), split(key_hat))]
    return Prepared(
        left,
        right,
        jnp.concatenate((values, values), axis=0),
        pltpu.roll(unit_hat * from_start, HEAD, 1),
        query_hat * from_start,
        spread(split(pull_hat * to_end)),
        jnp.concatenate(split(key_hat * to_end), axis=0),
        jnp.exp(end),
    )


def mixer_kernel(pairs, q_ref, k_ref, v_ref, r_ref, l_ref, g_ref, z_ref, local_ref, carry_ref):
    refs = (q_ref, k_ref, v_ref, r_ref, l_ref, g_ref)
    tokens = q_ref.shape[0]
    row, col = iota((tokens, tokens), 0), iota((tokens, tokens), 1)
    strict, upto, apart = row > col, row >= col, row ^ col
    first = iota((tokens, LANES), 1) < HEAD
    masks = Masks(
        ((iota((LANES, LANES), 0) < HEAD) == (iota((LANES, LANES), 1) < HEAD)).astype(BF16),
        upto.astype(BF16),
    )
    own_lanes = (first, jnp.logical_not(first))
    lanes = [slice(pair * LANES, (pair + 1) * LANES) for pair in range(pairs)]
    ready = [mixer_prepare(refs, part, masks) for part in lanes]
    heads = [(pair, head) for pair in range(pairs) for head in range(2)]

    scores = []
    for pair, head in heads:
        inside = jnp.concatenate((own_lanes[head], own_lanes[head]), axis=0)
        own = [jnp.where(inside, x, jnp.zeros_like(x)) for x in ready[pair].left]
        right = ready[pair].right
        scores.append(
            mxu(packed(own), packed((right[0], right[0])), ((1,), (1,)))
            + mxu(own[0], right[1], ((1,), (1,)))
        )
    mix_pull = [jnp.where(strict, s[:tokens, :tokens], 0.0) for s in scores]
    mix_key = [jnp.where(strict, s[:tokens, tokens:], 0.0) for s in scores]
    read_pull = [split(jnp.where(upto, s[tokens:, :tokens], 0.0)) for s in scores]
    read_key = [jnp.where(upto, s[tokens:, tokens:], 0.0) for s in scores]
    by_key = []
    for n, (pair, head) in enumerate(heads):
        both = [jnp.concatenate(p, axis=0) for p in zip(split(mix_key[n]), split(read_key[n]))]
        by_key.append(mxu(packed(both), ready[pair].values))

    identity = (row == col).astype(F32)
    inverse = [identity - jnp.where(apart < 2, m, 0.0) for m in mix_pull]
    size = 2
    while size < tokens:
        within = (apart >= size) & (apart < 2 * size)
        parts = [split(x) for x in inverse]
        edges = [split(jnp.where(within, m, 0.0)) for m in mix_pull]
        steps = [split(product(x, y)) for x, y in zip(parts, edges)]
        inverse = [x - product(y, z) for x, y, z in zip(inverse, steps, parts)]
        size *= 2

    answers, solved, outer = [], [], []
    for n, (pair, head) in enumerate(heads):
        sources = jnp.where(own_lanes[head], by_key[n][:tokens], ready[pair].starts)
        answers.append(split(product(split(inverse[n]), split(sources))))
    for n, (pair, head) in enumerate(heads):
        solved.append(product(read_pull[n], answers[n]))
        stacked = jnp.concatenate(answers[n], axis=0)
        outer.append(folded(mxu(stacked, ready[pair].pull_tail, ((0,), (0,)))))

    half = iota((HEAD, LANES), 1) < HEAD
    diagonal = (iota((HEAD, LANES), 1) % HEAD) == iota((HEAD, LANES), 0)
    for pair in range(pairs):
        one, two = 2 * pair, 2 * pair + 1
        local_ref[:, lanes[pair]] = jnp.where(
            first, by_key[one][tokens:] - solved[one], by_key[two][tokens:] - solved[two]
        )
        carry_ref[:, lanes[pair]] = ready[pair].query_now - pltpu.roll(
            jnp.where(first, solved[two], solved[one]), HEAD, 1
        )
        written = mxu(ready[pair].values, ready[pair].key_tail, ((0,), (0,)))
        z_ref[pair, :HEAD] = jnp.where(
            half, written[:HEAD] - outer[one][:HEAD], written[HEAD:] - outer[two][HEAD:]
        ).astype(BF16)
        changed = jnp.where(diagonal, ready[pair].decay_all - 1.0, 0.0) - jnp.where(
            half, outer[one][HEAD:], outer[two][:HEAD]
        )
        z_ref[pair, HEAD:] = changed.astype(BF16)


MESH = pl.DeviceIdType.MESH
GROUP_EPS = 0.00064
NORM_EPS = 1e-06
COLUMNS = 512


def block_diagonal(rows):
    first = iota(rows.shape, 1) < HEAD
    zero = jnp.zeros_like(rows)
    return jnp.concatenate((jnp.where(first, rows, zero), jnp.where(first, zero, rows)), axis=0)


def compose(earlier, later):
    turned = product(split(earlier), split(block_diagonal(later[HEAD:])))
    return turned + earlier + later


def prefixes(blocks):
    done, step = list(blocks), 1
    while step < len(done):
        for j in range(len(done)):
            if (j // step) % 2 == 1:
                done[j] = compose(done[j // step * step - 1], done[j])
        step *= 2
    return done


def joined_all(blocks):
    while len(blocks) > 1:
        pairs = [compose(*blocks[j : j + 2]) for j in range(0, len(blocks) - 1, 2)]
        blocks = pairs + (blocks[-1:] if len(blocks) % 2 else [])
    return blocks[0]


def remote(source, target, sends, receives, place):
    return pltpu.make_async_remote_copy(
        src_ref=source,
        dst_ref=target,
        send_sem=sends,
        recv_sem=receives,
        device_id=place,
        device_id_type=MESH,
    )


def member_copies(z, by_member, sent, got, part, parts):
    group, member, core = (lax.axis_index(a) for a in ("grp", "mem", "tp"))
    count = by_member.shape[0] // parts
    copies = []
    for offset in range(count):
        peer = part * count + lax.rem(member + offset, count)
        copy = remote(
            z.at[peer], by_member.at[member], sent.at[peer], got.at[member], (group, peer, core)
        )
        copies.append((peer != member, copy))
    return copies


def start_all(copies):
    for away, copy in copies:
        pl.when(away)(copy.start)


def sent_all(copies):
    for away, copy in copies:
        pl.when(away)(copy.wait_send)


def entering_states(z, by_member, by_group, total_ref, found, entered, sems):
    group, member, core = (lax.axis_index(a) for a in ("grp", "mem", "tp"))
    members, groups = by_member.shape[0], by_group.shape[0]
    got_1, sent_2, got_2, sent_3, got_3 = sems

    by_member[member] = z[member]
    for offset in range(1, members):
        peer = lax.rem(member + offset, members)
        remote(
            z.at[peer], by_member.at[peer], sent_3.at[offset], got_1.at[peer], (group, peer, core)
        ).wait_recv()
    inclusive = prefixes([by_member[j].astype(F32) for j in range(members)])
    total_ref[...] = inclusive[-1].astype(BF16)

    copies = []
    for offset in range(1, groups):
        peer = lax.rem(group + offset, groups)
        copy = remote(
            total_ref,
            by_group.at[group],
            sent_2.at[offset],
            got_2.at[group],
            (peer, member, core),
        )
        copy.start()
        copies.append(copy)
    maps = [spread(split(block_diagonal(inclusive[j][HEAD:]))) for j in range(members - 1)]
    by_group[group] = total_ref[...]
    for offset in range(1, groups):
        peer = lax.rem(group + offset, groups)
        remote(
            total_ref, by_group.at[peer], sent_2.at[offset], got_2.at[peer], (peer, member, core)
        ).wait_recv()
    before = [jnp.where(j < group, by_group[j].astype(F32), 0.0) for j in range(groups - 1)]
    start = joined_all(before)[:HEAD]
    parts = packed(split(start))
    found[0] = start.astype(BF16)
    for j in range(1, members):
        turned = folded(mxu(parts, maps[j - 1]))
        found[j] = (turned + start + inclusive[j - 1][:HEAD]).astype(BF16)

    for offset in range(1, members):
        peer = lax.rem(member + offset, members)
        copy = remote(
            found.at[peer],
            entered.at[member],
            sent_3.at[offset],
            got_3.at[member],
            (group, peer, core),
        )
        copy.start()
        copies.append(copy)
    entered[member] = found[member]
    for offset in range(1, members):
        peer = lax.rem(member + offset, members)
        remote(
            found.at[peer], entered.at[peer], sent_3.at[offset], got_3.at[peer], (group, peer, core)
        ).wait_recv()
    return copies


def normed_heads(local_ref, carry_ref, entered, gain_ref, normed):
    same_head = ((iota((LANES, LANES), 0) < HEAD) == (iota((LANES, LANES), 1) < HEAD)).astype(BF16)
    same_head = jnp.concatenate((same_head, same_head), axis=0)
    pairs = entered.shape[0]
    per_step = pairs // local_ref.shape[0]
    lanes = [slice(pair * LANES, (pair + 1) * LANES) for pair in range(pairs)]
    mixed = []
    for pair in range(pairs):
        state = block_diagonal(entered[pair])
        step, held = pair // per_step, lanes[pair % per_step]
        carry = packed(split(carry_ref[step, :, held]))
        read = mxu(carry, packed((state, state)), ((1,), (1,)))
        mixed.append(local_ref[step, :, held] + read)
    centred = [x - mxu(packed(split(x)), same_head) * (1.0 / HEAD) for x in mixed]
    variance = [mxu(packed(split(x * x)), same_head) * (1.0 / HEAD) for x in centred]
    for pair in range(pairs):
        scaled = centred[pair] * lax.rsqrt(variance[pair] + GROUP_EPS)
        normed[:, lanes[pair]] = (scaled * gain_ref[:, lanes[pair]].astype(F32)).astype(BF16)


def slot_map(routes_ref, experts, capacity):
    half = routes_ref.shape[1]
    shape = (experts * capacity, half)
    place = iota(shape, 0)
    expert, slot = place // capacity, place % capacity
    named = [routes_ref[k : k + 1, :] == expert for k in range(2)]
    chosen = (named[0] | named[1]).astype(F32)
    earlier = (iota((half, half), 0) < iota((half, half), 1)).astype(BF16)
    count = mxu(chosen.astype(BF16), earlier)
    return jnp.where(count == slot.astype(F32), chosen, 0.0), named


SP_TP = ("grp", "mem", "tp")
SP = ("grp", "mem")
STEPS = 2
BOUNDS = (0, 16, 32, 48, 64)
GROUPS = len(BOUNDS) - 1


def far_first(side):
    offsets = [(z, y, x) for z in range(side) for y in range(side) for x in range(side)]
    return sorted(offsets, key=lambda o: -sum(min(d, side - d) for d in o))


def layer_kernel(
    q_ref,
    k_ref,
    v_ref,
    r_ref,
    l_ref,
    g_ref,
    stream_ref,
    weight_ref,
    gate_ref,
    up_ref,
    down_ref,
    gain_ref,
    ffn_gain_ref,
    routes_ref,
    share_ref,
    out_ref,
    q,
    k,
    v,
    r,
    l,
    g,
    stream,
    weight,
    gate,
    up,
    down,
    z,
    local_read,
    carry_read,
    by_member,
    by_group,
    total_ref,
    found,
    entered,
    normed,
    partial,
    other,
    attended,
    dispatched,
    rows,
    hidden,
    part,
    part_got,
    back_out,
    back,
    in_sems,
    fetch_sems,
    sent_1,
    got_1,
    sent_2,
    got_2,
    sent_3,
    got_3,
    sent_4,
    got_4,
    row_sent,
    row_got,
    pass_sent,
    pass_got,
    part_sent,
    part_arrived,
    back_sent,
    back_got,
):
    group, member, core = (lax.axis_index(a) for a in ("grp", "mem", "tp"))
    members = lax.axis_size("mem")
    chips, experts = back.shape[1], dispatched.shape[0]
    capacity, width = rows.shape[2:]
    half_width = width // 2
    chip = group * members + member
    sibling = (group, member, 1 - core)

    def at(target, which):
        return (target // members, lax.rem(target, members), which)

    barrier = pltpu.get_barrier_semaphore()
    devices = 2 * chips

    def greet(offset, carry):
        peer = lax.rem(2 * chip + core + offset, devices)
        pl.semaphore_signal(
            barrier, inc=1, device_id=at(peer // 2, lax.rem(peer, 2)), device_id_type=MESH
        )
        return carry

    held = q.shape[2]
    loads = []
    for step in range(STEPS):
        lanes = pl.ds(step * held, held)
        for n, (source, target) in enumerate(
            ((q_ref, q), (k_ref, k), (v_ref, v), (r_ref, r), (l_ref, l), (g_ref, g))
        ):
            loads.append(
                pltpu.make_async_copy(source.at[:, lanes], target.at[step], in_sems.at[step, n])
            )
            loads[-1].start()
    depth = weight.shape[0]
    fetches = []
    for n, (source, target) in enumerate(
        (
            (stream_ref, stream),
            (weight_ref.at[pl.ds(core * depth, depth)], weight),
            (gate_ref.at[0], gate),
            (up_ref.at[0], up),
            (down_ref.at[0], down),
        )
    ):
        fetches.append(pltpu.make_async_copy(source, target, fetch_sems.at[n]))
    lax.fori_loop(1, devices, greet, 0)
    for copy in loads[: len(loads) // STEPS]:
        copy.wait()
    for copy in fetches:
        copy.start()

    pairs = z.shape[0] // STEPS

    def mix(step):
        mixer_kernel(
            pairs,
            *(ref.at[step] for ref in (q, k, v, r, l, g)),
            z.at[pl.ds(step * pairs, pairs)],
            local_read.at[step],
            carry_read.at[step],
        )

    mix(0)
    pl.semaphore_wait(barrier, devices - 1)
    early = member_copies(z, by_member, sent_1, got_1, 0, STEPS)
    start_all(early)
    for copy in loads[len(loads) // STEPS :]:
        copy.wait()
    mix(1)
    late = member_copies(z, by_member, sent_1, got_1, 1, STEPS)
    start_all(late)

    sems = (got_1, sent_2, got_2, sent_3, got_3)
    copies = entering_states(z, by_member, by_group, total_ref, found, entered, sems)
    normed_heads(local_read, carry_read, entered, gain_ref, normed)
    fetches[0].wait()
    fetches[1].wait()
    half = stream.shape[0]
    chunks = partial.shape[0]
    mine, theirs = pl.ds(core * half, half), pl.ds((1 - core) * half, half)
    shared = []
    for n in range(chunks):
        partial[n] = jnp.dot(
            normed[...], weight[:, n * COLUMNS : (n + 1) * COLUMNS], preferred_element_type=F32
        )
        shared.append(
            remote(partial.at[n, theirs], other.at[n], sent_4.at[n], got_4.at[n], sibling)
        )
        shared[-1].start()
    kept, named = slot_map(routes_ref, experts, capacity)
    picks = kept.astype(BF16)
    shares = kept * jnp.where(named[0], share_ref[0:1, :], share_ref[1:2, :])
    shares = jnp.concatenate(split(shares), axis=0)
    squares = jnp.zeros((half, 1), F32)
    for n in range(chunks):
        lanes = slice(n * COLUMNS, (n + 1) * COLUMNS)
        shared[n].wait_recv()
        block = stream[:, lanes].astype(F32) + (partial[n, mine] + other[n])
        attended[:, lanes] = block
        squares = squares + jnp.sum(block * block, axis=1, keepdims=True)
    scaling = lax.rsqrt(squares * (1.0 / width) + NORM_EPS)
    for n in range(chunks):
        lanes = slice(n * COLUMNS, (n + 1) * COLUMNS)
        ffn_in = attended[:, lanes] * scaling * ffn_gain_ref[:, lanes].astype(F32)
        sent_rows = mxu(picks, ffn_in.astype(BF16)).astype(BF16)
        dispatched[:, :, lanes] = sent_rows.reshape(experts, capacity, COLUMNS)

    side = round(chips ** (1 / 3))
    order = far_first(side)
    here = (chip // (side * side), chip // side % side, chip % side)

    def shifted(offset, sign):
        place = [lax.rem(h + side + sign * o, side) for h, o in zip(here, offset)]
        return (place[0] * side + place[1]) * side + place[2]

    rows[core, chips - 1] = dispatched[chip // 2]
    for n, offset in enumerate(order[:-1]):
        target = shifted(offset, 1)
        remote(
            dispatched.at[target // 2],
            rows.at[core, n],
            row_sent.at[sum(n >= b for b in BOUNDS[1:])],
            row_got.at[sum(n >= b for b in BOUNDS[1:])],
            at(target, core),
        ).start()
    for copy in fetches[2:]:
        copy.wait()

    def row_copies(step):
        start, stop = BOUNDS[step : step + 2]
        held = rows.at[core, pl.ds(start, min(stop, chips - 1) - start)]
        return remote(held, held, row_sent.at[step], row_got.at[step], sibling)

    def passing(step, which):
        start, stop = BOUNDS[step : step + 2]
        held = rows.at[which, pl.ds(start, stop - start)]
        return remote(held, held, pass_sent.at[step], pass_got.at[step], sibling)

    def taken_rows(step):
        start, stop = BOUNDS[step : step + 2]
        return slice(2 * start * capacity, 2 * stop * capacity)

    def part_copy(step):
        taken = taken_rows(step)
        taken = pl.ds(taken.start, taken.stop - taken.start)
        return remote(
            part.at[1 - core, taken],
            part_got.at[taken],
            part_sent.at[step],
            part_arrived.at[step],
            sibling,
        )

    def compute(step):
        start, stop = BOUNDS[step : step + 2]
        count = 2 * (stop - start) * capacity
        taken = rows[:, start:stop].reshape(count, width)
        inner = gate.shape[1]
        for begin in range(0, inner, 256):
            lanes = slice(begin, min(begin + 256, inner))
            gate_act = mxu(taken, gate[:, lanes])
            up_act = mxu(taken, up[:, lanes])
            hidden[:count, lanes] = (gate_act * jax.nn.sigmoid(gate_act) * up_act).astype(BF16)
        for which in range(2):
            for begin in range(0, half_width, COLUMNS):
                columns = slice(which * half_width + begin, which * half_width + begin + COLUMNS)
                part[which, taken_rows(step), begin : begin + COLUMNS] = mxu(
                    hidden[:count], down[:, columns]
                ).astype(BF16)

    def finish(step):
        part_copy(step).wait_recv()
        start, stop = BOUNDS[step : step + 2]
        total = part[core, taken_rows(step)].astype(F32) + part_got[taken_rows(step)].astype(F32)
        back_out[:, start:stop] = total.astype(BF16).reshape(2, stop - start, capacity, half_width)
        for n in range(start, stop):
            target = shifted(order[n], -1)
            for turn in range(2):
                which = 1 - core if turn == 0 else core
                if turn == 1 and not any(order[n]):
                    back[core, chip] = back_out[core, n]
                    continue
                remote(
                    back_out.at[which, n],
                    back.at[core, chip],
                    back_sent.at[step],
                    back_got.at[core],
                    at(target, which),
                ).start()

    for step in range(GROUPS):
        row_copies(step).wait_recv()
        passing(step, core).start()
        if step > 0:
            finish(step - 1)
        passing(step, 1 - core).wait_recv()
        compute(step)
        part_copy(step).start()
    finish(GROUPS - 1)

    def all_back(ref, sem_sent, sem_got):
        return remote(ref, ref, sem_sent, sem_got, sibling)

    for turn in range(2):
        which = 1 - core if turn == 0 else core
        all_back(back.at[which, pl.ds(0, chips - turn)], back_sent.at[0], back_got.at[which]).wait_recv()
    for which in range(2):
        lanes = slice(which * half_width, (which + 1) * half_width)
        both = back[which].reshape(experts, 2, capacity, half_width).astype(F32)
        whole = (both[:, 0] + both[:, 1]).astype(BF16).reshape(experts * capacity, half_width)
        mixture = mxu(shares, jnp.concatenate((whole, whole), axis=0), ((0,), (0,)))
        out_ref[:, lanes] = (attended[:, lanes] + mixture).astype(BF16)

    sent_all(early + late)
    for copy in copies + shared:
        copy.wait_send()
    for step in range(GROUPS):
        row_copies(step).wait_send()
        passing(step, core).wait_send()
        part_copy(step).wait_send()
        start, stop = BOUNDS[step : step + 2]
        last = 1 if step == GROUPS - 1 else 0
        for which, count in enumerate((stop - start, stop - start - last)):
            all_back(
                back_out.at[which, pl.ds(start, count)], back_sent.at[step], back_got.at[0]
            ).wait_send()


def local(
    stream_in,
    query_rows,
    key_rows,
    value_rows,
    removal_key,
    learn_pre,
    log_rate,
    norm_gain,
    out_weight,
    ffn_gain,
    routes,
    route_weight,
    expert_gate,
    expert_up,
    expert_down,
):
    half, width = stream_in.shape
    tokens, own_width = query_rows.shape
    chips = lax.axis_size(("grp", "mem"))
    members, groups = lax.axis_size("mem"), lax.axis_size("grp")
    experts = chips // 2
    capacity = 2 * routes.shape[1] * half // experts
    inner = expert_gate.shape[2]
    held = own_width // STEPS
    pairs = own_width // LANES
    chunks = width // COLUMNS
    taken = 2 * max(b - a for a, b in zip(BOUNDS, BOUNDS[1:])) * capacity
    vmem = pl.BlockSpec(memory_space=pltpu.VMEM)
    hbm = pl.BlockSpec(memory_space=pl.ANY)
    dma = pltpu.SemaphoreType.DMA
    return pl.pallas_call(
        layer_kernel,
        in_specs=[hbm] * 11 + [vmem] * 4,
        out_specs=vmem,
        out_shape=jax.ShapeDtypeStruct((half, width), BF16),
        scratch_shapes=[pltpu.VMEM((STEPS, tokens, held), BF16)] * 5
        + [
            pltpu.VMEM((STEPS, tokens, held), F32),
            pltpu.VMEM((half, width), BF16),
            pltpu.VMEM((width // 2, width), BF16),
            pltpu.VMEM((width, inner), BF16),
            pltpu.VMEM((width, inner), BF16),
            pltpu.VMEM((inner, width), BF16),
            pltpu.VMEM((pairs, 2 * HEAD, LANES), BF16),
            pltpu.VMEM((STEPS, tokens, held), F32),
            pltpu.VMEM((STEPS, tokens, held), F32),
            pltpu.VMEM((members, 2 * HEAD, LANES), BF16),
            pltpu.VMEM((groups, 2 * HEAD, LANES), BF16),
            pltpu.VMEM((2 * HEAD, LANES), BF16),
            pltpu.VMEM((members, HEAD, LANES), BF16),
            pltpu.VMEM((members, HEAD, LANES), BF16),
            pltpu.VMEM((tokens, own_width), BF16),
            pltpu.VMEM((chunks, tokens, COLUMNS), F32),
            pltpu.VMEM((chunks, half, COLUMNS), F32),
            pltpu.VMEM((half, width), F32),
            pltpu.VMEM((experts, capacity, width), BF16),
            pltpu.VMEM((2, chips, capacity, width), BF16),
            pltpu.VMEM((taken, inner), BF16),
            pltpu.VMEM((2, 2 * chips * capacity, width // 2), BF16),
            pltpu.VMEM((2 * chips * capacity, width // 2), BF16),
            pltpu.VMEM((2, chips, capacity, width // 2), BF16),
            pltpu.VMEM((2, chips, capacity, width // 2), BF16),
            dma((STEPS, 6)),
            dma((5,)),
            dma((members,)),
            dma((members,)),
            dma((groups,)),
            dma((groups,)),
            dma((members,)),
            dma((members,)),
            dma((chunks,)),
            dma((chunks,)),
        ]
        + [dma((GROUPS,))] * 7
        + [dma((2,))],
        compiler_params=pltpu.CompilerParams(
            collective_id=0, has_side_effects=True, vmem_limit_bytes=63 * 1024 * 1024
        ),
        name="layer",
    )(
        query_rows,
        key_rows,
        value_rows,
        removal_key,
        learn_pre,
        log_rate,
        stream_in,
        out_weight,
        expert_gate,
        expert_up,
        expert_down,
        norm_gain.reshape(1, -1),
        ffn_gain.reshape(1, -1),
        routes.T,
        route_weight.T,
    )


def solution(mesh):
    sp = mesh.shape["sp"]
    groups = 1
    while groups * groups < sp:
        groups *= 2
    torus = Mesh(
        mesh.devices.reshape(sp // groups, groups, mesh.shape["tp"]), ("grp", "mem", "tp")
    )
    return jax.shard_map(
        local,
        mesh=torus,
        in_specs=(
            P(SP_TP, None),
            P(SP, "tp"),
            P(SP, "tp"),
            P(SP, "tp"),
            P(SP, "tp"),
            P(SP, "tp"),
            P(SP, "tp"),
            P("tp"),
            P(),
            P(),
            P(SP_TP, None),
            P(SP_TP, None),
            P(SP, None, "tp"),
            P(SP, None, "tp"),
            P(SP, "tp", None),
        ),
        out_specs=P(SP_TP, None),
        check_vma=False,
    )
```

```python
from typing import NamedTuple

import jax
import jax.numpy as jnp
from jax import lax
from jax.experimental import pallas as pl
from jax.experimental.pallas import tpu as pltpu
from jax.sharding import Mesh
from jax.sharding import PartitionSpec as P

HEAD = 64
LANES = 128
F32 = jnp.float32
BF16 = jnp.bfloat16
UNIT_EPS = 1e-06


def split(x):
    high = x.astype(BF16)
    return high, (x - high.astype(F32)).astype(BF16)


def mxu(x, y, dims=((1,), (0,))):
    return lax.dot_general(x, y, (dims, ((), ())), preferred_element_type=F32)


def packed(x):
    return jnp.concatenate(x, axis=1)


def spread(y):
    high, low = y
    top = jnp.concatenate((high, low), axis=1)
    return jnp.concatenate((top, top), axis=0)


def folded(z):
    half = z.shape[1] // 2
    return z[:, :half] + z[:, half:]


def product(x, y):
    return folded(mxu(packed(x), spread(y)))


def iota(shape, dim):
    return lax.broadcasted_iota(jnp.int32, shape, dim)


class Masks(NamedTuple):
    same_head: jax.Array
    lower: jax.Array


class Prepared(NamedTuple):
    left: list
    right: list
    values: jax.Array
    starts: jax.Array
    query_now: jax.Array
    pull_tail: jax.Array
    key_tail: jax.Array
    decay_all: jax.Array


def mixer_prepare(refs, lanes, masks):
    q_ref, k_ref, v_ref, r_ref, l_ref, g_ref = refs
    tokens = q_ref.shape[0]
    removal = r_ref[:, lanes].astype(F32)
    squares = split(removal * removal)
    total = mxu(packed(squares), jnp.concatenate((masks.same_head, masks.same_head), axis=0))
    unit = removal * lax.rsqrt(total + UNIT_EPS)
    pull = unit * jax.nn.sigmoid(l_ref[:, lanes].astype(F32))
    log_decay = -jnp.exp(g_ref[:, lanes])
    high = log_decay.astype(BF16)
    rest = log_decay - high.astype(F32)
    mid = rest.astype(BF16)
    low = (rest - mid.astype(F32)).astype(BF16)
    stacked = jnp.concatenate((packed((high, mid)), packed((low, jnp.zeros_like(low)))), axis=0)
    cumul = folded(mxu(packed((masks.lower, masks.lower)), stacked))
    middle = cumul[tokens // 2 - 1 : tokens // 2]
    end = cumul[tokens - 1 : tokens]
    grown = jnp.exp(middle - cumul)
    faded = jnp.exp(cumul - middle)
    unit_hat = unit * jnp.exp(cumul - log_decay - middle)
    query_hat = q_ref[:, lanes].astype(F32) * faded
    pull_hat = pull * grown
    key_hat = k_ref[:, lanes].astype(F32) * grown
    from_start = jnp.exp(middle)
    to_end = jnp.exp(end - middle)
    values = v_ref[:, lanes]
    left = [jnp.concatenate(p, axis=0) for p in zip(split(unit_hat), split(query_hat))]
    right = [jnp.concatenate(p, axis=0) for p in zip(split(pull_hat), split(key_hat))]
    return Prepared(
        left,
        right,
        jnp.concatenate((values, values), axis=0),
        pltpu.roll(unit_hat * from_start, HEAD, 1),
        query_hat * from_start,
        spread(split(pull_hat * to_end)),
        jnp.concatenate(split(key_hat * to_end), axis=0),
        jnp.exp(end),
    )


def mixer_kernel(pairs, q_ref, k_ref, v_ref, r_ref, l_ref, g_ref, z_ref, local_ref, carry_ref):
    refs = (q_ref, k_ref, v_ref, r_ref, l_ref, g_ref)
    tokens = q_ref.shape[0]
    row, col = iota((tokens, tokens), 0), iota((tokens, tokens), 1)
    strict, upto, apart = row > col, row >= col, row ^ col
    first = iota((tokens, LANES), 1) < HEAD
    masks = Masks(
        ((iota((LANES, LANES), 0) < HEAD) == (iota((LANES, LANES), 1) < HEAD)).astype(BF16),
        upto.astype(BF16),
    )
    own_lanes = (first, jnp.logical_not(first))
    lanes = [slice(pair * LANES, (pair + 1) * LANES) for pair in range(pairs)]
    ready = [mixer_prepare(refs, part, masks) for part in lanes]
    heads = [(pair, head) for pair in range(pairs) for head in range(2)]

    scores = []
    for pair, head in heads:
        inside = jnp.concatenate((own_lanes[head], own_lanes[head]), axis=0)
        own = [jnp.where(inside, x, jnp.zeros_like(x)) for x in ready[pair].left]
        right = ready[pair].right
        scores.append(
            mxu(packed(own), packed((right[0], right[0])), ((1,), (1,)))
            + mxu(own[0], right[1], ((1,), (1,)))
        )
    mix_pull = [jnp.where(strict, s[:tokens, :tokens], 0.0) for s in scores]
    mix_key = [jnp.where(strict, s[:tokens, tokens:], 0.0) for s in scores]
    read_pull = [split(jnp.where(upto, s[tokens:, :tokens], 0.0)) for s in scores]
    read_key = [jnp.where(upto, s[tokens:, tokens:], 0.0) for s in scores]
    by_key = []
    for n, (pair, head) in enumerate(heads):
        both = [jnp.concatenate(p, axis=0) for p in zip(split(mix_key[n]), split(read_key[n]))]
        by_key.append(mxu(packed(both), ready[pair].values))

    identity = (row == col).astype(F32)
    inverse = [identity - jnp.where(apart < 2, m, 0.0) for m in mix_pull]
    size = 2
    while size < tokens:
        within = (apart >= size) & (apart < 2 * size)
        parts = [split(x) for x in inverse]
        edges = [split(jnp.where(within, m, 0.0)) for m in mix_pull]
        steps = [split(product(x, y)) for x, y in zip(parts, edges)]
        inverse = [x - product(y, z) for x, y, z in zip(inverse, steps, parts)]
        size *= 2

    answers, solved, outer = [], [], []
    for n, (pair, head) in enumerate(heads):
        sources = jnp.where(own_lanes[head], by_key[n][:tokens], ready[pair].starts)
        answers.append(split(product(split(inverse[n]), split(sources))))
    for n, (pair, head) in enumerate(heads):
        solved.append(product(read_pull[n], answers[n]))
        stacked = jnp.concatenate(answers[n], axis=0)
        outer.append(folded(mxu(stacked, ready[pair].pull_tail, ((0,), (0,)))))

    half = iota((HEAD, LANES), 1) < HEAD
    diagonal = (iota((HEAD, LANES), 1) % HEAD) == iota((HEAD, LANES), 0)
    for pair in range(pairs):
        one, two = 2 * pair, 2 * pair + 1
        local_ref[:, lanes[pair]] = jnp.where(
            first, by_key[one][tokens:] - solved[one], by_key[two][tokens:] - solved[two]
        )
        carry_ref[:, lanes[pair]] = ready[pair].query_now - pltpu.roll(
            jnp.where(first, solved[two], solved[one]), HEAD, 1
        )
        written = mxu(ready[pair].values, ready[pair].key_tail, ((0,), (0,)))
        z_ref[pair, :HEAD] = jnp.where(
            half, written[:HEAD] - outer[one][:HEAD], written[HEAD:] - outer[two][HEAD:]
        ).astype(BF16)
        changed = jnp.where(diagonal, ready[pair].decay_all - 1.0, 0.0) - jnp.where(
            half, outer[one][HEAD:], outer[two][:HEAD]
        )
        z_ref[pair, HEAD:] = changed.astype(BF16)


MESH = pl.DeviceIdType.MESH
GROUP_EPS = 0.00064
NORM_EPS = 1e-06
COLUMNS = 512


def block_diagonal(rows):
    first = iota(rows.shape, 1) < HEAD
    zero = jnp.zeros_like(rows)
    return jnp.concatenate((jnp.where(first, rows, zero), jnp.where(first, zero, rows)), axis=0)


def compose(earlier, later):
    turned = product(split(earlier), split(block_diagonal(later[HEAD:])))
    return turned + earlier + later


def prefixes(blocks):
    done, step = list(blocks), 1
    while step < len(done):
        for j in range(len(done)):
            if (j // step) % 2 == 1:
                done[j] = compose(done[j // step * step - 1], done[j])
        step *= 2
    return done


def joined_all(blocks):
    while len(blocks) > 1:
        pairs = [compose(*blocks[j : j + 2]) for j in range(0, len(blocks) - 1, 2)]
        blocks = pairs + (blocks[-1:] if len(blocks) % 2 else [])
    return blocks[0]


def remote(source, target, sends, receives, place):
    return pltpu.make_async_remote_copy(
        src_ref=source,
        dst_ref=target,
        send_sem=sends,
        recv_sem=receives,
        device_id=place,
        device_id_type=MESH,
    )


def member_copies(z, by_member, sent, got, part, parts):
    group, member, core = (lax.axis_index(a) for a in ("grp", "mem", "tp"))
    count = by_member.shape[0] // parts
    copies = []
    for offset in range(count):
        peer = part * count + lax.rem(member + offset, count)
        copy = remote(
            z.at[peer], by_member.at[member], sent.at[peer], got.at[member], (group, peer, core)
        )
        copies.append((peer != member, copy))
    return copies


def start_all(copies):
    for away, copy in copies:
        pl.when(away)(copy.start)


def sent_all(copies):
    for away, copy in copies:
        pl.when(away)(copy.wait_send)


def entering_states(z, by_member, by_group, total_ref, found, entered, sems):
    group, member, core = (lax.axis_index(a) for a in ("grp", "mem", "tp"))
    members, groups = by_member.shape[0], by_group.shape[0]
    got_1, sent_2, got_2, sent_3, got_3 = sems

    by_member[member] = z[member]
    for offset in range(1, members):
        peer = lax.rem(member + offset, members)
        remote(
            z.at[peer], by_member.at[peer], sent_3.at[offset], got_1.at[peer], (group, peer, core)
        ).wait_recv()
    inclusive = prefixes([by_member[j].astype(F32) for j in range(members)])
    total_ref[...] = inclusive[-1].astype(BF16)

    copies = []
    for offset in range(1, groups):
        peer = lax.rem(group + offset, groups)
        copy = remote(
            total_ref,
            by_group.at[group],
            sent_2.at[offset],
            got_2.at[group],
            (peer, member, core),
        )
        copy.start()
        copies.append(copy)
    maps = [spread(split(block_diagonal(inclusive[j][HEAD:]))) for j in range(members - 1)]
    by_group[group] = total_ref[...]
    for offset in range(1, groups):
        peer = lax.rem(group + offset, groups)
        remote(
            total_ref, by_group.at[peer], sent_2.at[offset], got_2.at[peer], (peer, member, core)
        ).wait_recv()
    before = [jnp.where(j < group, by_group[j].astype(F32), 0.0) for j in range(groups - 1)]
    start = joined_all(before)[:HEAD]
    parts = packed(split(start))
    found[0] = start.astype(BF16)
    for j in range(1, members):
        turned = folded(mxu(parts, maps[j - 1]))
        found[j] = (turned + start + inclusive[j - 1][:HEAD]).astype(BF16)

    for offset in range(1, members):
        peer = lax.rem(member + offset, members)
        copy = remote(
            found.at[peer],
            entered.at[member],
            sent_3.at[offset],
            got_3.at[member],
            (group, peer, core),
        )
        copy.start()
        copies.append(copy)
    entered[member] = found[member]
    for offset in range(1, members):
        peer = lax.rem(member + offset, members)
        remote(
            found.at[peer], entered.at[peer], sent_3.at[offset], got_3.at[peer], (group, peer, core)
        ).wait_recv()
    return copies


def normed_heads(local_ref, carry_ref, entered, gain_ref, normed):
    same_head = ((iota((LANES, LANES), 0) < HEAD) == (iota((LANES, LANES), 1) < HEAD)).astype(BF16)
    same_head = jnp.concatenate((same_head, same_head), axis=0)
    pairs = entered.shape[0]
    per_step = pairs // local_ref.shape[0]
    lanes = [slice(pair * LANES, (pair + 1) * LANES) for pair in range(pairs)]
    mixed = []
    for pair in range(pairs):
        state = block_diagonal(entered[pair])
        step, held = pair // per_step, lanes[pair % per_step]
        carry = packed(split(carry_ref[step, :, held]))
        read = mxu(carry, packed((state, state)), ((1,), (1,)))
        mixed.append(local_ref[step, :, held] + read)
    centred = [x - mxu(packed(split(x)), same_head) * (1.0 / HEAD) for x in mixed]
    variance = [mxu(packed(split(x * x)), same_head) * (1.0 / HEAD) for x in centred]
    for pair in range(pairs):
        scaled = centred[pair] * lax.rsqrt(variance[pair] + GROUP_EPS)
        normed[:, lanes[pair]] = (scaled * gain_ref[pair : pair + 1].astype(F32)).astype(BF16)


def slot_map(routes_ref, experts, capacity):
    half = routes_ref.shape[1]
    shape = (experts * capacity, half)
    place = iota(shape, 0)
    expert, slot = place // capacity, place % capacity
    named = [routes_ref[k : k + 1, :] == expert for k in range(2)]
    chosen = (named[0] | named[1]).astype(F32)
    earlier = (iota((half, half), 0) < iota((half, half), 1)).astype(BF16)
    count = mxu(chosen.astype(BF16), earlier)
    return jnp.where(count == slot.astype(F32), chosen, 0.0), named


SP_TP = ("grp", "mem", "tp")
SP = ("grp", "mem")
STEPS = 2
BOUNDS = (0, 16, 32, 48, 64)
GROUPS = len(BOUNDS) - 1


def far_first(side):
    offsets = [(z, y, x) for z in range(side) for y in range(side) for x in range(side)]
    return sorted(offsets, key=lambda o: -sum(min(d, side - d) for d in o))


def layer_kernel(
    q_ref,
    k_ref,
    v_ref,
    r_ref,
    l_ref,
    g_ref,
    stream_ref,
    weight_ref,
    gate_ref,
    up_ref,
    down_ref,
    gain_ref,
    ffn_gain_ref,
    routes_ref,
    share_ref,
    out_ref,
    q,
    k,
    v,
    r,
    l,
    g,
    stream,
    weight,
    gate,
    up,
    down,
    z,
    local_read,
    carry_read,
    by_member,
    by_group,
    total_ref,
    found,
    entered,
    normed,
    partial,
    other,
    attended,
    dispatched,
    rows,
    hidden,
    part,
    part_got,
    back_out,
    back,
    in_sems,
    fetch_sems,
    sent_1,
    got_1,
    sent_2,
    got_2,
    sent_3,
    got_3,
    sent_4,
    got_4,
    row_sent,
    row_got,
    pass_sent,
    pass_got,
    part_sent,
    part_arrived,
    back_sent,
    back_got,
):
    group, member, core = (lax.axis_index(a) for a in ("grp", "mem", "tp"))
    members = lax.axis_size("mem")
    chips, experts = back.shape[0], dispatched.shape[0]
    capacity, width = rows.shape[2:]
    half_width = width // 2
    chip = group * members + member
    sibling = (group, member, 1 - core)

    def at(target, which):
        return (target // members, lax.rem(target, members), which)

    barrier = pltpu.get_barrier_semaphore()

    def greet(offset, carry):
        peer = at(lax.rem(chip + offset, chips), core)
        pl.semaphore_signal(barrier, inc=1, device_id=peer, device_id_type=MESH)
        return carry

    held = q.shape[2]
    loads = []
    for step in range(STEPS):
        lanes = pl.ds(step * held, held)
        for n, (source, target) in enumerate(
            ((q_ref, q), (k_ref, k), (v_ref, v), (r_ref, r), (l_ref, l), (g_ref, g))
        ):
            loads.append(
                pltpu.make_async_copy(source.at[:, lanes], target.at[step], in_sems.at[step, n])
            )
            loads[-1].start()
    depth = weight.shape[0]
    fetches = []
    for n, (source, target) in enumerate(
        (
            (stream_ref, stream),
            (weight_ref.at[pl.ds(core * depth, depth)], weight),
            (gate_ref.at[0], gate),
            (up_ref.at[0], up),
            (down_ref.at[0], down),
        )
    ):
        fetches.append(pltpu.make_async_copy(source, target, fetch_sems.at[n]))
    lax.fori_loop(1, chips, greet, 0)
    pl.semaphore_signal(barrier, inc=1, device_id=sibling, device_id_type=MESH)
    for copy in loads[: len(loads) // STEPS]:
        copy.wait()
    for copy in fetches:
        copy.start()

    pairs = z.shape[0] // STEPS

    def mix(step):
        mixer_kernel(
            pairs,
            *(ref.at[step] for ref in (q, k, v, r, l, g)),
            z.at[pl.ds(step * pairs, pairs)],
            local_read.at[step],
            carry_read.at[step],
        )

    mix(0)
    pl.semaphore_wait(barrier, chips)
    early = member_copies(z, by_member, sent_1, got_1, 0, STEPS)
    start_all(early)
    for copy in loads[len(loads) // STEPS :]:
        copy.wait()
    mix(1)
    late = member_copies(z, by_member, sent_1, got_1, 1, STEPS)
    start_all(late)

    sems = (got_1, sent_2, got_2, sent_3, got_3)
    copies = entering_states(z, by_member, by_group, total_ref, found, entered, sems)
    normed_heads(local_read, carry_read, entered, gain_ref, normed)
    fetches[0].wait()
    fetches[1].wait()
    half = stream.shape[0]
    chunks = partial.shape[0]
    mine, theirs = pl.ds(core * half, half), pl.ds((1 - core) * half, half)
    shared = []
    for n in range(chunks):
        partial[n] = jnp.dot(
            normed[...], weight[:, n * COLUMNS : (n + 1) * COLUMNS], preferred_element_type=F32
        )
        shared.append(
            remote(partial.at[n, theirs], other.at[n], sent_4.at[n], got_4.at[n], sibling)
        )
        shared[-1].start()
    kept, named = slot_map(routes_ref, experts, capacity)
    picks = kept.astype(BF16)
    shares = kept * jnp.where(named[0], share_ref[0:1, :], share_ref[1:2, :])
    shares = jnp.concatenate(split(shares), axis=0)
    squares = jnp.zeros((half, 1), F32)
    for n in range(chunks):
        lanes = slice(n * COLUMNS, (n + 1) * COLUMNS)
        shared[n].wait_recv()
        block = stream[:, lanes].astype(F32) + (partial[n, mine] + other[n])
        attended[:, lanes] = block
        squares = squares + jnp.sum(block * block, axis=1, keepdims=True)
    scaling = lax.rsqrt(squares * (1.0 / width) + NORM_EPS)
    for n in range(chunks):
        lanes = slice(n * COLUMNS, (n + 1) * COLUMNS)
        gains = [ffn_gain_ref[r : r + 1] for r in range(lanes.start // LANES, lanes.stop // LANES)]
        ffn_in = attended[:, lanes] * scaling * packed([x.astype(F32) for x in gains])
        sent_rows = mxu(picks, ffn_in.astype(BF16)).astype(BF16)
        dispatched[:, :, lanes] = sent_rows.reshape(experts, capacity, COLUMNS)

    side = round(chips ** (1 / 3))
    order = far_first(side)
    here = (chip // (side * side), chip // side % side, chip % side)

    def shifted(offset, sign):
        place = [lax.rem(h + side + sign * o, side) for h, o in zip(here, offset)]
        return (place[0] * side + place[1]) * side + place[2]

    rows[core, chips - 1] = dispatched[chip // 2]
    for n, offset in enumerate(order[:-1]):
        target = shifted(offset, 1)
        remote(
            dispatched.at[target // 2],
            rows.at[core, n],
            row_sent.at[sum(n >= b for b in BOUNDS[1:])],
            row_got.at[sum(n >= b for b in BOUNDS[1:])],
            at(target, core),
        ).start()
    for copy in fetches[2:]:
        copy.wait()

    def row_copies(step):
        start, stop = BOUNDS[step : step + 2]
        held = rows.at[core, pl.ds(start, min(stop, chips - 1) - start)]
        return remote(held, held, row_sent.at[step], row_got.at[step], sibling)

    def passing(step, which):
        start, stop = BOUNDS[step : step + 2]
        held = rows.at[which, pl.ds(start, stop - start)]
        return remote(held, held, pass_sent.at[step], pass_got.at[step], sibling)

    def taken_rows(step):
        start, stop = BOUNDS[step : step + 2]
        return slice(start * capacity, stop * capacity)

    def part_copy(step):
        taken = taken_rows(step)
        taken = pl.ds(taken.start, taken.stop - taken.start)
        return remote(
            part.at[1 - core, taken],
            part_got.at[taken],
            part_sent.at[step],
            part_arrived.at[step],
            sibling,
        )

    def compute(step):
        start, stop = BOUNDS[step : step + 2]
        count = (stop - start) * capacity
        taken = rows[:, start:stop].reshape(2 * count, width)
        inner = gate.shape[1]
        for begin in range(0, inner, 256):
            size = min(256, inner - begin)
            lanes = slice(begin, begin + size)
            if size == 256:
                gate_act, up_act = mxu(taken, gate[:, lanes]), mxu(taken, up[:, lanes])
            else:
                both = mxu(taken, packed((gate[:, lanes], up[:, lanes])))
                gate_act, up_act = both[:, :size], both[:, size:]
            hidden[: 2 * count, lanes] = (gate_act * jax.nn.sigmoid(gate_act) * up_act).astype(BF16)
        for begin in range(0, width, COLUMNS):
            columns = slice(begin, begin + COLUMNS)
            block = mxu(hidden[: 2 * count], down[:, columns]).astype(BF16)
            part[0, taken_rows(step), columns] = block[:count]
            part[1, taken_rows(step), columns] = block[count:]

    def finish(step):
        part_copy(step).wait_recv()
        start, stop = BOUNDS[step : step + 2]
        total = part[core, taken_rows(step)].astype(F32) + part_got[taken_rows(step)].astype(F32)
        back_out[start:stop] = total.astype(BF16).reshape(stop - start, capacity, width)
        for n in range(start, stop):
            if not any(order[n]):
                back[chip] = back_out[n]
                continue
            remote(
                back_out.at[n],
                back.at[chip],
                back_sent.at[step],
                back_got,
                at(shifted(order[n], -1), core),
            ).start()

    for step in range(GROUPS):
        row_copies(step).wait_recv()
        passing(step, core).start()
        if step > 0:
            finish(step - 1)
        passing(step, 1 - core).wait_recv()
        compute(step)
        part_copy(step).start()
    finish(GROUPS - 1)

    def all_back(ref, sem_sent, sem_got):
        return remote(ref, ref, sem_sent, sem_got, sibling)

    all_back(back.at[pl.ds(0, chips - 1)], back_sent.at[0], back_got).wait_recv()
    for which in range(2):
        lanes = slice(which * half_width, (which + 1) * half_width)
        both = back[:, :, lanes].reshape(experts, 2, capacity, half_width).astype(F32)
        whole = (both[:, 0] + both[:, 1]).astype(BF16).reshape(experts * capacity, half_width)
        mixture = mxu(shares, jnp.concatenate((whole, whole), axis=0), ((0,), (0,)))
        out_ref[:, lanes] = (attended[:, lanes] + mixture).astype(BF16)

    sent_all(early + late)
    for copy in copies + shared:
        copy.wait_send()
    for step in range(GROUPS):
        row_copies(step).wait_send()
        passing(step, core).wait_send()
        part_copy(step).wait_send()
        start, stop = BOUNDS[step : step + 2]
        last = 1 if step == GROUPS - 1 else 0
        count = stop - start - last
        all_back(back_out.at[pl.ds(start, count)], back_sent.at[step], back_got).wait_send()


def local(
    stream_in,
    query_rows,
    key_rows,
    value_rows,
    removal_key,
    learn_pre,
    log_rate,
    norm_gain,
    out_weight,
    ffn_gain,
    routes,
    route_weight,
    expert_gate,
    expert_up,
    expert_down,
):
    half, width = stream_in.shape
    tokens, own_width = query_rows.shape
    chips = lax.axis_size(("grp", "mem"))
    members, groups = lax.axis_size("mem"), lax.axis_size("grp")
    experts = chips // 2
    capacity = 2 * routes.shape[1] * half // experts
    inner = expert_gate.shape[2]
    held = own_width // STEPS
    pairs = own_width // LANES
    chunks = width // COLUMNS
    taken = 2 * max(b - a for a, b in zip(BOUNDS, BOUNDS[1:])) * capacity
    vmem = pl.BlockSpec(memory_space=pltpu.VMEM)
    hbm = pl.BlockSpec(memory_space=pl.ANY)
    dma = pltpu.SemaphoreType.DMA
    return pl.pallas_call(
        layer_kernel,
        in_specs=[hbm] * 11 + [vmem] * 4,
        out_specs=vmem,
        out_shape=jax.ShapeDtypeStruct((half, width), BF16),
        scratch_shapes=[pltpu.VMEM((STEPS, tokens, held), BF16)] * 5
        + [
            pltpu.VMEM((STEPS, tokens, held), F32),
            pltpu.VMEM((half, width), BF16),
            pltpu.VMEM((width // 2, width), BF16),
            pltpu.VMEM((width, inner), BF16),
            pltpu.VMEM((width, inner), BF16),
            pltpu.VMEM((inner, width), BF16),
            pltpu.VMEM((pairs, 2 * HEAD, LANES), BF16),
            pltpu.VMEM((STEPS, tokens, held), F32),
            pltpu.VMEM((STEPS, tokens, held), F32),
            pltpu.VMEM((members, 2 * HEAD, LANES), BF16),
            pltpu.VMEM((groups, 2 * HEAD, LANES), BF16),
            pltpu.VMEM((2 * HEAD, LANES), BF16),
            pltpu.VMEM((members, HEAD, LANES), BF16),
            pltpu.VMEM((members, HEAD, LANES), BF16),
            pltpu.VMEM((tokens, own_width), BF16),
            pltpu.VMEM((chunks, tokens, COLUMNS), F32),
            pltpu.VMEM((chunks, half, COLUMNS), F32),
            pltpu.VMEM((half, width), F32),
            pltpu.VMEM((experts, capacity, width), BF16),
            pltpu.VMEM((2, chips, capacity, width), BF16),
            pltpu.VMEM((taken, inner), BF16),
            pltpu.VMEM((2, chips * capacity, width), BF16),
            pltpu.VMEM((chips * capacity, width), BF16),
            pltpu.VMEM((chips, capacity, width), BF16),
            pltpu.VMEM((chips, capacity, width), BF16),
            dma((STEPS, 6)),
            dma((5,)),
            dma((members,)),
            dma((members,)),
            dma((groups,)),
            dma((groups,)),
            dma((members,)),
            dma((members,)),
            dma((chunks,)),
            dma((chunks,)),
        ]
        + [dma((GROUPS,))] * 7
        + [dma],
        compiler_params=pltpu.CompilerParams(
            collective_id=0, has_side_effects=True, vmem_limit_bytes=63 * 1024 * 1024
        ),
        name="layer",
    )(
        query_rows,
        key_rows,
        value_rows,
        removal_key,
        learn_pre,
        log_rate,
        stream_in,
        out_weight,
        expert_gate,
        expert_up,
        expert_down,
        norm_gain.reshape(-1, LANES),
        ffn_gain.reshape(-1, LANES),
        routes.T,
        route_weight.T,
    )


def solution(mesh):
    sp = mesh.shape["sp"]
    groups = 1
    while groups * groups < sp:
        groups *= 2
    torus = Mesh(
        mesh.devices.reshape(sp // groups, groups, mesh.shape["tp"]), ("grp", "mem", "tp")
    )
    return jax.shard_map(
        local,
        mesh=torus,
        in_specs=(
            P(SP_TP, None),
            P(SP, "tp"),
            P(SP, "tp"),
            P(SP, "tp"),
            P(SP, "tp"),
            P(SP, "tp"),
            P(SP, "tp"),
            P("tp"),
            P(),
            P(),
            P(SP_TP, None),
            P(SP_TP, None),
            P(SP, None, "tp"),
            P(SP, None, "tp"),
            P(SP, "tp", None),
        ),
        out_specs=P(SP_TP, None),
        check_vma=False,
    )
```

```python
from typing import NamedTuple

import jax
import jax.numpy as jnp
from jax import lax
from jax.experimental import pallas as pl
from jax.experimental.pallas import tpu as pltpu
from jax.sharding import Mesh
from jax.sharding import PartitionSpec as P

HEAD = 64
LANES = 128
F32 = jnp.float32
BF16 = jnp.bfloat16
UNIT_EPS = 1e-06


def split(x):
    high = x.astype(BF16)
    return high, (x - high.astype(F32)).astype(BF16)


def mxu(x, y, dims=((1,), (0,))):
    return lax.dot_general(x, y, (dims, ((), ())), preferred_element_type=F32)


def packed(x):
    return jnp.concatenate(x, axis=1)


def spread(y):
    high, low = y
    top = jnp.concatenate((high, low), axis=1)
    return jnp.concatenate((top, top), axis=0)


def folded(z):
    half = z.shape[1] // 2
    return z[:, :half] + z[:, half:]


def product(x, y):
    return folded(mxu(packed(x), spread(y)))


def iota(shape, dim):
    return lax.broadcasted_iota(jnp.int32, shape, dim)


class Masks(NamedTuple):
    same_head: jax.Array
    lower: jax.Array


class Prepared(NamedTuple):
    left: list
    right: list
    values: jax.Array
    starts: jax.Array
    query_now: jax.Array
    pull_tail: jax.Array
    key_tail: jax.Array
    decay_all: jax.Array


def mixer_prepare(refs, lanes, masks):
    q_ref, k_ref, v_ref, r_ref, l_ref, g_ref = refs
    tokens = q_ref.shape[0]
    removal = r_ref[:, lanes].astype(F32)
    squares = split(removal * removal)
    total = mxu(packed(squares), jnp.concatenate((masks.same_head, masks.same_head), axis=0))
    unit = removal * lax.rsqrt(total + UNIT_EPS)
    pull = unit * jax.nn.sigmoid(l_ref[:, lanes].astype(F32))
    log_decay = -jnp.exp(g_ref[:, lanes])
    high = log_decay.astype(BF16)
    rest = log_decay - high.astype(F32)
    mid = rest.astype(BF16)
    low = (rest - mid.astype(F32)).astype(BF16)
    stacked = jnp.concatenate((packed((high, mid)), packed((low, jnp.zeros_like(low)))), axis=0)
    cumul = folded(mxu(packed((masks.lower, masks.lower)), stacked))
    middle = cumul[tokens // 2 - 1 : tokens // 2]
    end = cumul[tokens - 1 : tokens]
    grown = jnp.exp(middle - cumul)
    faded = jnp.exp(cumul - middle)
    unit_hat = unit * jnp.exp(cumul - log_decay - middle)
    query_hat = q_ref[:, lanes].astype(F32) * faded
    pull_hat = pull * grown
    key_hat = k_ref[:, lanes].astype(F32) * grown
    from_start = jnp.exp(middle)
    to_end = jnp.exp(end - middle)
    values = v_ref[:, lanes]
    left = [jnp.concatenate(p, axis=0) for p in zip(split(unit_hat), split(query_hat))]
    right = [jnp.concatenate(p, axis=0) for p in zip(split(pull_hat), split(key_hat))]
    return Prepared(
        left,
        right,
        jnp.concatenate((values, values), axis=0),
        pltpu.roll(unit_hat * from_start, HEAD, 1),
        query_hat * from_start,
        spread(split(pull_hat * to_end)),
        jnp.concatenate(split(key_hat * to_end), axis=0),
        jnp.exp(end),
    )


def mixer_kernel(pairs, q_ref, k_ref, v_ref, r_ref, l_ref, g_ref, z_ref, local_ref, carry_ref):
    refs = (q_ref, k_ref, v_ref, r_ref, l_ref, g_ref)
    tokens = q_ref.shape[0]
    row, col = iota((tokens, tokens), 0), iota((tokens, tokens), 1)
    strict, upto, apart = row > col, row >= col, row ^ col
    first = iota((tokens, LANES), 1) < HEAD
    masks = Masks(
        ((iota((LANES, LANES), 0) < HEAD) == (iota((LANES, LANES), 1) < HEAD)).astype(BF16),
        upto.astype(BF16),
    )
    own_lanes = (first, jnp.logical_not(first))
    lanes = [slice(pair * LANES, (pair + 1) * LANES) for pair in range(pairs)]
    ready = [mixer_prepare(refs, part, masks) for part in lanes]
    heads = [(pair, head) for pair in range(pairs) for head in range(2)]

    scores = []
    for pair, head in heads:
        inside = jnp.concatenate((own_lanes[head], own_lanes[head]), axis=0)
        own = [jnp.where(inside, x, jnp.zeros_like(x)) for x in ready[pair].left]
        right = ready[pair].right
        scores.append(
            mxu(packed(own), packed((right[0], right[0])), ((1,), (1,)))
            + mxu(own[0], right[1], ((1,), (1,)))
        )
    mix_pull = [jnp.where(strict, s[:tokens, :tokens], 0.0) for s in scores]
    mix_key = [jnp.where(strict, s[:tokens, tokens:], 0.0) for s in scores]
    read_pull = [split(jnp.where(upto, s[tokens:, :tokens], 0.0)) for s in scores]
    read_key = [jnp.where(upto, s[tokens:, tokens:], 0.0) for s in scores]
    by_key = []
    for n, (pair, head) in enumerate(heads):
        both = [jnp.concatenate(p, axis=0) for p in zip(split(mix_key[n]), split(read_key[n]))]
        by_key.append(mxu(packed(both), ready[pair].values))

    identity = (row == col).astype(F32)
    inverse = [identity - jnp.where(apart < 2, m, 0.0) for m in mix_pull]
    size = 2
    while size < tokens:
        within = (apart >= size) & (apart < 2 * size)
        parts = [split(x) for x in inverse]
        edges = [split(jnp.where(within, m, 0.0)) for m in mix_pull]
        steps = [split(product(x, y)) for x, y in zip(parts, edges)]
        inverse = [x - product(y, z) for x, y, z in zip(inverse, steps, parts)]
        size *= 2

    answers, solved, outer = [], [], []
    for n, (pair, head) in enumerate(heads):
        sources = jnp.where(own_lanes[head], by_key[n][:tokens], ready[pair].starts)
        answers.append(split(product(split(inverse[n]), split(sources))))
    for n, (pair, head) in enumerate(heads):
        solved.append(product(read_pull[n], answers[n]))
        stacked = jnp.concatenate(answers[n], axis=0)
        outer.append(folded(mxu(stacked, ready[pair].pull_tail, ((0,), (0,)))))

    half = iota((HEAD, LANES), 1) < HEAD
    diagonal = (iota((HEAD, LANES), 1) % HEAD) == iota((HEAD, LANES), 0)
    for pair in range(pairs):
        one, two = 2 * pair, 2 * pair + 1
        local_ref[:, lanes[pair]] = jnp.where(
            first, by_key[one][tokens:] - solved[one], by_key[two][tokens:] - solved[two]
        )
        carry_ref[:, lanes[pair]] = ready[pair].query_now - pltpu.roll(
            jnp.where(first, solved[two], solved[one]), HEAD, 1
        )
        written = mxu(ready[pair].values, ready[pair].key_tail, ((0,), (0,)))
        z_ref[pair, :HEAD] = jnp.where(
            half, written[:HEAD] - outer[one][:HEAD], written[HEAD:] - outer[two][HEAD:]
        ).astype(BF16)
        changed = jnp.where(diagonal, ready[pair].decay_all - 1.0, 0.0) - jnp.where(
            half, outer[one][HEAD:], outer[two][:HEAD]
        )
        z_ref[pair, HEAD:] = changed.astype(BF16)


MESH = pl.DeviceIdType.MESH
GROUP_EPS = 0.00064
NORM_EPS = 1e-06
COLUMNS = 512


def block_diagonal(rows):
    first = iota(rows.shape, 1) < HEAD
    zero = jnp.zeros_like(rows)
    return jnp.concatenate((jnp.where(first, rows, zero), jnp.where(first, zero, rows)), axis=0)


def compose(earlier, later):
    turned = product(split(earlier), split(block_diagonal(later[HEAD:])))
    return turned + earlier + later


def prefixes(blocks):
    done, step = list(blocks), 1
    while step < len(done):
        for j in range(len(done)):
            if (j // step) % 2 == 1:
                done[j] = compose(done[j // step * step - 1], done[j])
        step *= 2
    return done


def joined_all(blocks):
    while len(blocks) > 1:
        pairs = [compose(*blocks[j : j + 2]) for j in range(0, len(blocks) - 1, 2)]
        blocks = pairs + (blocks[-1:] if len(blocks) % 2 else [])
    return blocks[0]


def remote(source, target, sends, receives, place):
    return pltpu.make_async_remote_copy(
        src_ref=source,
        dst_ref=target,
        send_sem=sends,
        recv_sem=receives,
        device_id=place,
        device_id_type=MESH,
    )


def member_copies(z, by_member, sent, got, part, parts):
    group, member, core = (lax.axis_index(a) for a in ("grp", "mem", "tp"))
    count = by_member.shape[0] // parts
    copies = []
    for offset in range(count):
        peer = part * count + lax.rem(member + offset, count)
        copy = remote(
            z.at[peer], by_member.at[member], sent.at[peer], got.at[member], (group, peer, core)
        )
        copies.append((peer != member, copy))
    return copies


def start_all(copies):
    for away, copy in copies:
        pl.when(away)(copy.start)


def sent_all(copies):
    for away, copy in copies:
        pl.when(away)(copy.wait_send)


def entering_states(z, by_member, by_group, total_ref, found, entered, sems):
    group, member, core = (lax.axis_index(a) for a in ("grp", "mem", "tp"))
    members, groups = by_member.shape[0], by_group.shape[0]
    got_1, sent_2, got_2, sent_3, got_3 = sems

    by_member[member] = z[member]
    for offset in range(1, members):
        peer = lax.rem(member + offset, members)
        remote(
            z.at[peer], by_member.at[peer], sent_3.at[offset], got_1.at[peer], (group, peer, core)
        ).wait_recv()
    inclusive = prefixes([by_member[j].astype(F32) for j in range(members)])
    total_ref[...] = inclusive[-1].astype(BF16)

    copies = []
    for offset in range(1, groups):
        peer = lax.rem(group + offset, groups)
        copy = remote(
            total_ref,
            by_group.at[group],
            sent_2.at[offset],
            got_2.at[group],
            (peer, member, core),
        )
        copy.start()
        copies.append(copy)
    maps = [spread(split(block_diagonal(inclusive[j][HEAD:]))) for j in range(members - 1)]
    by_group[group] = total_ref[...]
    for offset in range(1, groups):
        peer = lax.rem(group + offset, groups)
        remote(
            total_ref, by_group.at[peer], sent_2.at[offset], got_2.at[peer], (peer, member, core)
        ).wait_recv()
    before = [jnp.where(j < group, by_group[j].astype(F32), 0.0) for j in range(groups - 1)]
    start = joined_all(before)[:HEAD]
    parts = packed(split(start))
    found[0] = start.astype(BF16)
    for j in range(1, members):
        turned = folded(mxu(parts, maps[j - 1]))
        found[j] = (turned + start + inclusive[j - 1][:HEAD]).astype(BF16)

    for offset in range(1, members):
        peer = lax.rem(member + offset, members)
        copy = remote(
            found.at[peer],
            entered.at[member],
            sent_3.at[offset],
            got_3.at[member],
            (group, peer, core),
        )
        copy.start()
        copies.append(copy)
    entered[member] = found[member]
    for offset in range(1, members):
        peer = lax.rem(member + offset, members)
        remote(
            found.at[peer], entered.at[peer], sent_3.at[offset], got_3.at[peer], (group, peer, core)
        ).wait_recv()
    return copies


def normed_heads(local_ref, carry_ref, entered, gain_ref, normed):
    same_head = ((iota((LANES, LANES), 0) < HEAD) == (iota((LANES, LANES), 1) < HEAD)).astype(BF16)
    same_head = jnp.concatenate((same_head, same_head), axis=0)
    pairs = entered.shape[0]
    per_step = pairs // local_ref.shape[0]
    lanes = [slice(pair * LANES, (pair + 1) * LANES) for pair in range(pairs)]
    mixed = []
    for pair in range(pairs):
        state = block_diagonal(entered[pair])
        step, held = pair // per_step, lanes[pair % per_step]
        carry = packed(split(carry_ref[step, :, held]))
        read = mxu(carry, packed((state, state)), ((1,), (1,)))
        mixed.append(local_ref[step, :, held] + read)
    centred = [x - mxu(packed(split(x)), same_head) * (1.0 / HEAD) for x in mixed]
    variance = [mxu(packed(split(x * x)), same_head) * (1.0 / HEAD) for x in centred]
    for pair in range(pairs):
        scaled = centred[pair] * lax.rsqrt(variance[pair] + GROUP_EPS)
        normed[:, lanes[pair]] = (scaled * gain_ref[pair : pair + 1].astype(F32)).astype(BF16)


def slot_map(routes_ref, experts, capacity):
    half = routes_ref.shape[1]
    shape = (experts * capacity, half)
    place = iota(shape, 0)
    expert, slot = place // capacity, place % capacity
    named = [routes_ref[k : k + 1, :] == expert for k in range(2)]
    chosen = (named[0] | named[1]).astype(F32)
    earlier = (iota((half, half), 0) < iota((half, half), 1)).astype(BF16)
    count = mxu(chosen.astype(BF16), earlier)
    return jnp.where(count == slot.astype(F32), chosen, 0.0), named


SP_TP = ("grp", "mem", "tp")
SP = ("grp", "mem")
STEPS = 2
BOUNDS = (0, 12, 28, 44, 56, 64)
GROUPS = len(BOUNDS) - 1


def far_first(side):
    offsets = [(z, y, x) for z in range(side) for y in range(side) for x in range(side)]
    return sorted(offsets, key=lambda o: -sum(min(d, side - d) for d in o))


def layer_kernel(
    q_ref,
    k_ref,
    v_ref,
    r_ref,
    l_ref,
    g_ref,
    stream_ref,
    weight_ref,
    gate_ref,
    up_ref,
    down_ref,
    gain_ref,
    ffn_gain_ref,
    routes_ref,
    share_ref,
    out_ref,
    q,
    k,
    v,
    r,
    l,
    g,
    stream,
    weight,
    gate,
    up,
    down,
    z,
    local_read,
    carry_read,
    by_member,
    by_group,
    total_ref,
    found,
    entered,
    normed,
    partial,
    other,
    attended,
    dispatched,
    rows,
    hidden,
    part,
    part_got,
    back_out,
    back,
    share_rows,
    share_of,
    in_sems,
    fetch_sems,
    sent_1,
    got_1,
    sent_2,
    got_2,
    sent_3,
    got_3,
    sent_4,
    got_4,
    row_sent,
    row_got,
    pass_sent,
    pass_got,
    part_sent,
    part_arrived,
    back_sent,
    back_got,
):
    group, member, core = (lax.axis_index(a) for a in ("grp", "mem", "tp"))
    members = lax.axis_size("mem")
    chips, experts = back.shape[0], dispatched.shape[0]
    capacity, width = rows.shape[2:]
    chip = group * members + member
    sibling = (group, member, 1 - core)

    def at(target, which):
        return (lax.div(target, members), lax.rem(target, members), which)

    barrier = pltpu.get_barrier_semaphore()

    held = q.shape[2]
    loads = []
    for step in range(STEPS):
        lanes = pl.ds(step * held, held)
        for n, (source, target) in enumerate(
            ((q_ref, q), (k_ref, k), (v_ref, v), (r_ref, r), (l_ref, l), (g_ref, g))
        ):
            loads.append(
                pltpu.make_async_copy(source.at[:, lanes], target.at[step], in_sems.at[step, n])
            )
            loads[-1].start()
    depth = weight.shape[0]
    fetches = []
    for n, (source, target) in enumerate(
        (
            (stream_ref, stream),
            (weight_ref.at[pl.ds(core * depth, depth)], weight),
            (gate_ref.at[0], gate),
            (up_ref.at[0], up),
            (down_ref.at[0], down),
        )
    ):
        fetches.append(pltpu.make_async_copy(source, target, fetch_sems.at[n]))
    for peer in [at(lax.rem(chip + offset, chips), core) for offset in range(1, chips)] + [sibling]:
        pl.semaphore_signal(barrier, inc=1, device_id=peer, device_id_type=MESH)
    for copy in loads[: len(loads) // STEPS]:
        copy.wait()
    for copy in fetches:
        copy.start()

    pairs = z.shape[0] // STEPS

    def mix(step):
        mixer_kernel(
            pairs,
            *(ref.at[step] for ref in (q, k, v, r, l, g)),
            z.at[pl.ds(step * pairs, pairs)],
            local_read.at[step],
            carry_read.at[step],
        )

    mix(0)
    pl.semaphore_wait(barrier, chips)
    early = member_copies(z, by_member, sent_1, got_1, 0, STEPS)
    start_all(early)
    for copy in loads[len(loads) // STEPS :]:
        copy.wait()
    mix(1)
    late = member_copies(z, by_member, sent_1, got_1, 1, STEPS)
    start_all(late)

    sems = (got_1, sent_2, got_2, sent_3, got_3)
    copies = entering_states(z, by_member, by_group, total_ref, found, entered, sems)
    normed_heads(local_read, carry_read, entered, gain_ref, normed)
    fetches[0].wait()
    fetches[1].wait()
    half = stream.shape[0]
    chunks = partial.shape[0]
    mine, theirs = pl.ds(core * half, half), pl.ds((1 - core) * half, half)
    shared = []
    for n in range(chunks):
        partial[n] = jnp.dot(
            normed[...], weight[:, n * COLUMNS : (n + 1) * COLUMNS], preferred_element_type=F32
        )
        shared.append(
            remote(partial.at[n, theirs], other.at[n], sent_4.at[n], got_4.at[n], sibling)
        )
        shared[-1].start()
    kept, named = slot_map(routes_ref, experts, capacity)
    picks = kept.astype(BF16)
    share_rows[...] = kept * jnp.where(named[0], share_ref[0:1, :], share_ref[1:2, :])
    squares = jnp.zeros((half, 1), F32)
    for n in range(chunks):
        lanes = slice(n * COLUMNS, (n + 1) * COLUMNS)
        shared[n].wait_recv()
        block = stream[:, lanes].astype(F32) + (partial[n, mine] + other[n])
        attended[:, lanes] = block
        squares = squares + jnp.sum(block * block, axis=1, keepdims=True)
    scaling = lax.rsqrt(squares * (1.0 / width) + NORM_EPS)
    for n in range(chunks):
        lanes = slice(n * COLUMNS, (n + 1) * COLUMNS)
        gains = [ffn_gain_ref[r : r + 1] for r in range(lanes.start // LANES, lanes.stop // LANES)]
        ffn_in = attended[:, lanes] * scaling * packed([x.astype(F32) for x in gains])
        sent_rows = mxu(picks, ffn_in.astype(BF16)).astype(BF16)
        dispatched[:, :, lanes] = sent_rows.reshape(experts, capacity, COLUMNS)

    side = round(chips ** (1 / 3))
    order = far_first(side)
    here = (chip // (side * side), chip // side % side, chip % side)

    def shifted(offset, sign):
        place = [lax.rem(h + side + sign * o, side) for h, o in zip(here, offset)]
        return (place[0] * side + place[1]) * side + place[2]

    for n, offset in enumerate(order[:-1]):
        target = shifted(offset, 1)
        remote(
            dispatched.at[lax.div(target, 2)],
            rows.at[core, n],
            row_sent.at[sum(n >= b for b in BOUNDS[1:])],
            row_got.at[sum(n >= b for b in BOUNDS[1:])],
            at(target, core),
        ).start()
    rows[core, chips - 1] = dispatched[chip // 2]
    for n, offset in enumerate(order):
        expert = lax.div(shifted(offset, 1), 2)
        share_of[n * capacity : (n + 1) * capacity] = share_rows[
            pl.ds(pl.multiple_of(expert * capacity, capacity), capacity)
        ]
    for copy in fetches[2:]:
        copy.wait()

    def row_copies(step):
        start, stop = BOUNDS[step : step + 2]
        held = rows.at[core, pl.ds(start, min(stop, chips - 1) - start)]
        return remote(held, held, row_sent.at[step], row_got.at[step], sibling)

    def passing(step, which):
        start, stop = BOUNDS[step : step + 2]
        held = rows.at[which, pl.ds(start, stop - start)]
        return remote(held, held, pass_sent.at[step], pass_got.at[step], sibling)

    def taken_rows(step):
        start, stop = BOUNDS[step : step + 2]
        return slice(start * capacity, stop * capacity)

    def part_copy(step):
        taken = taken_rows(step)
        taken = pl.ds(taken.start, taken.stop - taken.start)
        return remote(
            part.at[1 - core, taken],
            part_got.at[taken],
            part_sent.at[step],
            part_arrived.at[step],
            sibling,
        )

    def compute(step):
        start, stop = BOUNDS[step : step + 2]
        count = (stop - start) * capacity
        taken = rows[:, start:stop].reshape(2 * count, width)
        inner = gate.shape[1]
        for begin in range(0, inner, 256):
            size = min(256, inner - begin)
            lanes = slice(begin, begin + size)
            if size == 256:
                gate_act, up_act = mxu(taken, gate[:, lanes]), mxu(taken, up[:, lanes])
            else:
                both = mxu(taken, packed((gate[:, lanes], up[:, lanes])))
                gate_act, up_act = both[:, :size], both[:, size:]
            hidden[: 2 * count, lanes] = (gate_act * jax.nn.sigmoid(gate_act) * up_act).astype(BF16)
        for begin in range(0, width, COLUMNS):
            columns = slice(begin, begin + COLUMNS)
            block = mxu(hidden[: 2 * count], down[:, columns]).astype(BF16)
            part[0, taken_rows(step), columns] = block[:count]
            part[1, taken_rows(step), columns] = block[count:]

    def finish(step):
        part_copy(step).wait_recv()
        start, stop = BOUNDS[step : step + 2]
        total = part[core, taken_rows(step)].astype(F32) + part_got[taken_rows(step)].astype(F32)
        back_out[start:stop] = total.astype(BF16).reshape(stop - start, capacity, width)
        for n in range(start, stop):
            if not any(order[n]):
                back[n] = back_out[n]
                continue
            remote(
                back_out.at[n],
                back.at[n],
                back_sent.at[step],
                back_got.at[step],
                at(shifted(order[n], -1), core),
            ).start()

    for step in range(GROUPS):
        row_copies(step).wait_recv()
        passing(step, core).start()
        if step > 0:
            finish(step - 1)
        passing(step, 1 - core).wait_recv()
        compute(step)
        part_copy(step).start()
    finish(GROUPS - 1)

    def all_back(ref, sem_sent, sem_got):
        return remote(ref, ref, sem_sent, sem_got, sibling)

    for step in range(GROUPS):
        start, stop = BOUNDS[step : step + 2]
        held = back.at[pl.ds(start, min(stop, chips - 1) - start)]
        all_back(held, back_sent.at[step], back_got.at[step]).wait_recv()
        weights = jnp.concatenate(split(share_of[start * capacity : stop * capacity]), axis=0)
        for begin in range(0, width, COLUMNS):
            lanes = slice(begin, begin + COLUMNS)
            block = back[start:stop, :, lanes].reshape((stop - start) * capacity, COLUMNS)
            total = attended[:, lanes] + mxu(
                weights, jnp.concatenate((block, block), axis=0), ((0,), (0,))
            )
            if step < GROUPS - 1:
                attended[:, lanes] = total
            else:
                out_ref[:, lanes] = total.astype(BF16)

    sent_all(early + late)
    for copy in copies + shared:
        copy.wait_send()
    for step in range(GROUPS):
        row_copies(step).wait_send()
        passing(step, core).wait_send()
        part_copy(step).wait_send()
        start, stop = BOUNDS[step : step + 2]
        last = 1 if step == GROUPS - 1 else 0
        count = stop - start - last
        sent = back_out.at[pl.ds(start, count)]
        all_back(sent, back_sent.at[step], back_got.at[step]).wait_send()


def local(
    stream_in,
    query_rows,
    key_rows,
    value_rows,
    removal_key,
    learn_pre,
    log_rate,
    norm_gain,
    out_weight,
    ffn_gain,
    routes,
    route_weight,
    expert_gate,
    expert_up,
    expert_down,
):
    half, width = stream_in.shape
    tokens, own_width = query_rows.shape
    chips = lax.axis_size(("grp", "mem"))
    members, groups = lax.axis_size("mem"), lax.axis_size("grp")
    experts = chips // 2
    capacity = 2 * routes.shape[1] * half // experts
    inner = expert_gate.shape[2]
    held = own_width // STEPS
    pairs = own_width // LANES
    chunks = width // COLUMNS
    taken = 2 * max(b - a for a, b in zip(BOUNDS, BOUNDS[1:])) * capacity
    vmem = pl.BlockSpec(memory_space=pltpu.VMEM)
    hbm = pl.BlockSpec(memory_space=pl.ANY)
    dma = pltpu.SemaphoreType.DMA
    return pl.pallas_call(
        layer_kernel,
        in_specs=[hbm] * 11 + [vmem] * 4,
        out_specs=vmem,
        out_shape=jax.ShapeDtypeStruct((half, width), BF16),
        scratch_shapes=[pltpu.VMEM((STEPS, tokens, held), BF16)] * 5
        + [
            pltpu.VMEM((STEPS, tokens, held), F32),
            pltpu.VMEM((half, width), BF16),
            pltpu.VMEM((width // 2, width), BF16),
            pltpu.VMEM((width, inner), BF16),
            pltpu.VMEM((width, inner), BF16),
            pltpu.VMEM((inner, width), BF16),
            pltpu.VMEM((pairs, 2 * HEAD, LANES), BF16),
            pltpu.VMEM((STEPS, tokens, held), F32),
            pltpu.VMEM((STEPS, tokens, held), F32),
            pltpu.VMEM((members, 2 * HEAD, LANES), BF16),
            pltpu.VMEM((groups, 2 * HEAD, LANES), BF16),
            pltpu.VMEM((2 * HEAD, LANES), BF16),
            pltpu.VMEM((members, HEAD, LANES), BF16),
            pltpu.VMEM((members, HEAD, LANES), BF16),
            pltpu.VMEM((tokens, own_width), BF16),
            pltpu.VMEM((chunks, tokens, COLUMNS), F32),
            pltpu.VMEM((chunks, half, COLUMNS), F32),
            pltpu.VMEM((half, width), F32),
            pltpu.VMEM((experts, capacity, width), BF16),
            pltpu.VMEM((2, chips, capacity, width), BF16),
            pltpu.VMEM((taken, inner), BF16),
            pltpu.VMEM((2, chips * capacity, width), BF16),
            pltpu.VMEM((chips * capacity, width), BF16),
            pltpu.VMEM((chips, capacity, width), BF16),
            pltpu.VMEM((chips, capacity, width), BF16),
            pltpu.VMEM((experts * capacity, half), F32),
            pltpu.VMEM((chips * capacity, half), F32),
            dma((STEPS, 6)),
            dma((5,)),
            dma((members,)),
            dma((members,)),
            dma((groups,)),
            dma((groups,)),
            dma((members,)),
            dma((members,)),
            dma((chunks,)),
            dma((chunks,)),
        ]
        + [dma((GROUPS,))] * 8,
        compiler_params=pltpu.CompilerParams(
            collective_id=0, has_side_effects=True, vmem_limit_bytes=63 * 1024 * 1024
        ),
        name="layer",
    )(
        query_rows,
        key_rows,
        value_rows,
        removal_key,
        learn_pre,
        log_rate,
        stream_in,
        out_weight,
        expert_gate,
        expert_up,
        expert_down,
        norm_gain.reshape(-1, LANES),
        ffn_gain.reshape(-1, LANES),
        routes.T,
        route_weight.T,
    )


def solution(mesh):
    sp = mesh.shape["sp"]
    groups = 1
    while groups * groups < sp:
        groups *= 2
    torus = Mesh(
        mesh.devices.reshape(sp // groups, groups, mesh.shape["tp"]), ("grp", "mem", "tp")
    )
    return jax.shard_map(
        local,
        mesh=torus,
        in_specs=(
            P(SP_TP, None),
            P(SP, "tp"),
            P(SP, "tp"),
            P(SP, "tp"),
            P(SP, "tp"),
            P(SP, "tp"),
            P(SP, "tp"),
            P("tp"),
            P(),
            P(),
            P(SP_TP, None),
            P(SP_TP, None),
            P(SP, None, "tp"),
            P(SP, None, "tp"),
            P(SP, "tp", None),
        ),
        out_specs=P(SP_TP, None),
        check_vma=False,
    )
```
